256 devices in a mesh: grp: 4 (over y, x), ep: 32 (over z), tp: 2 (over core).
Axes of the slice: x: 2, y: 2, z: 32, core: 2. Of those that a mesh axis runs over, the one named last changes fastest.
The devices are a block of a 4x8x32 slice.
Arguments:
- tokens: bfloat16 [65536, 2048], P(('grp', 'ep', 'tp')), parts along dimension 0, may hold values from -6 to 6
- norm_gain: float32 [2048], replicated, may hold values from 0.1 to 1.9
- expert_ids: int32 [65536, 2], P(('grp', 'ep', 'tp')), parts along dimension 0, may hold values from 0 to 31, all different within a row; in each aligned block of 256 rows (0 to 255, 256 to 511, ...) at most 24 rows name the same one
- route_weights: float32 [65536, 2], P(('grp', 'ep', 'tp')), parts along dimension 0, may hold values from 0.05 to 1
- w_gate: bfloat16 [32, 2048, 1024], P('ep', None, 'tp'), may hold values from -0.125 to 0.125
- w_up: bfloat16 [32, 2048, 1024], P('ep', None, 'tp'), may hold values from -0.125 to 0.125
- w_down: bfloat16 [32, 1024, 2048], P('ep', 'tp'), may hold values from -0.1875 to 0.1875
Outputs:
- mixed: bfloat16 [65536, 2048], P(('grp', 'ep', 'tp')), parts along dimension 0
The draws below stay inside these ranges and needn't reach their ends.
There are 4 independent parts, one for each index of `grp`. The reference program is written for one: setup_inputs(seed, part) draws one part's arguments, and reference() takes and returns one part's arrays. A program takes and returns all parts, laid end to end along the dimension named above; an argument that names none is the same for every part. Nothing has to cross between parts.
Inputs may be any that keep to these rules, and one draw needn't show every extreme that they name: `expert_ids`: each row names 2 different experts. Among the rows of one device no expert is named more than 24 times, and in every draw some expert is named exactly 24 times by the rows of some device.
All inputs are finite; a program needn't handle non-finite values.
Results may differ from the reference program's by a relative error of at most 0.0071.
Values may be sent and summed in bfloat16 or wider, within the bound.
A program may use at most 128 MiB of HBM per device.

```python
import math
import jax
import jax.numpy as jnp
import numpy as np
from jax import lax

D = 2048
DE = 1024
TOP_K = 2
TOK_DEV = 256
EXPERTS = 32
TOKENS = 16384
CAP = 24


def block_scale(own_key, shape, pieces, low, top_value):
    def one(axis_at, blocks):
        heights = jax.random.uniform(jax.random.fold_in(jax.random.fold_in(own_key, 6), axis_at), (blocks,), jnp.float32, low / len(pieces), top_value / len(pieces))
        return jnp.repeat(jnp.exp(heights), shape[axis_at] // blocks).reshape((-1,) + (1,) * (len(shape) - axis_at - 1))

    factor_of = one(*pieces[0])
    for cut in pieces[1:]:
        factor_of = factor_of * one(*cut)
    return factor_of


def assign_block(own_key, own, number, rows, amount, top, most, skew):
    ranking = jax.random.permutation(own_key, amount)
    crowded, usual = shares(amount, rows * top, most, skew, True), shares(amount, rows * top, most, skew, False)
    places = jnp.arange(amount)

    def named(lengths, rotation):
        used = int((lengths > 0).sum())
        fixed = max(1, used // 4)
        moved = fixed + (places - fixed + rotation * (used - fixed)) % max(1, amount - fixed)
        return jnp.zeros((amount,), jnp.int32).at[ranking[jnp.where(places < fixed, places, moved)]].set(jnp.asarray(lengths, jnp.int32))

    lengths = jnp.where(number % 4 == 0, named(crowded, number // 4), named(usual, number - number // 4 - 1))
    mixed = jax.random.permutation(jax.random.fold_in(own, 3), amount)
    donor, taker = mixed[0:amount // 2 * 2:2], mixed[1:amount // 2 * 2:2]
    margin = jnp.minimum(lengths[donor] - 1, most - lengths[taker]) // 2
    margin = jnp.where((donor == ranking[0]) | (taker == ranking[0]) | (lengths[taker] == 0), 0, jnp.maximum(margin, 0))
    moved = jax.random.randint(jax.random.fold_in(own, 4), (amount // 2,), 0, 1 << 20) % (margin + 1)
    lengths = lengths.at[donor].add(-moved).at[taker].add(moved)
    items = jnp.searchsorted(jnp.cumsum(lengths), jnp.arange(rows * top), side="right").astype(jnp.int32)
    table = items.reshape(top, rows).T
    table = table[jax.random.permutation(jax.random.fold_in(own, 1), rows)]
    rotation = jax.random.randint(jax.random.fold_in(own, 2), (rows, 1), 0, top)
    return jnp.take_along_axis(table, (jnp.arange(top)[None, :] + rotation) % top, axis=1)


def shares(count, total, reach, lean, full):
    portions = [(1 << 20) // math.isqrt(grade ** lean) + 1 for grade in range(1, count + 1)]
    largest = reach if full else min(reach, max(-(-total // count), total * portions[0] // sum(portions)))
    least = 1 if total - largest >= count - 1 else 0
    given, surplus = [largest] + [least] * (count - 1), total - largest - least * (count - 1)
    while surplus > 0:
        candidates = [i for i in range(1, count) if given[i] < largest] or [i for i in range(1, count) if given[i] < reach]
        whole, budget = sum([portions[i] for i in candidates]), surplus
        for i in candidates:
            addition = min(reach - given[i], max(1, budget * portions[i] // whole), surplus)
            given[i] = given[i] + addition
            surplus = surplus - addition
    return np.array(given)


def centred(stream_key, shape, deviation, reach, shards=(), kind=jnp.bfloat16):
    entries = jax.random.normal(stream_key, shape, jnp.float32) * deviation
    if len(shards) > 0:
        entries = block_scale(stream_key, shape, shards, -0.22, 0.18) * entries
    return jnp.clip(entries, min=-reach, max=reach).astype(kind)


def setup_inputs(seed: int = 0, part: int = 0) -> dict:
    arg_keys = jax.random.split(jax.random.key(seed), 8)
    part_splits = jax.random.split(jax.random.fold_in(arg_keys[7], part), 8)
    tokens = centred(part_splits[0], (TOKENS, D), 1.0, 6.0, ((0, 64),))
    norm_gain = jnp.clip(1.0 + 0.18 * jax.random.normal(arg_keys[1], (D,), jnp.float32), 0.1, 1.9)
    expert_ids_keys = jax.random.split(jax.random.fold_in(part_splits[2], 1), TOKENS // TOK_DEV)
    expert_ids_turns = jax.random.permutation(jax.random.fold_in(part_splits[2], 3), TOKENS // TOK_DEV)
    expert_ids = jax.vmap(lambda own, number: assign_block(jax.random.fold_in(part_splits[2], 2), own, number, TOK_DEV, EXPERTS, TOP_K, CAP, 2))(expert_ids_keys, expert_ids_turns).reshape((TOKENS, TOP_K))
    route_weights = jnp.clip(jnp.exp(math.log(1.0) - 2.9957323 * jax.random.uniform(part_splits[3], (TOKENS, TOP_K), jnp.float32) ** block_scale(part_splits[3], (TOKENS, TOP_K), ((0, 64),), -0.2, 0.2)), 0.05, 1.0)
    w_gate = centred(arg_keys[4], (EXPERTS, D, DE), D ** -0.5, 0.125, ((0, 32), (2, 2)))
    w_up = centred(arg_keys[5], (EXPERTS, D, DE), D ** -0.5, 0.125, ((0, 32), (2, 2)))
    w_down = centred(arg_keys[6], (EXPERTS, DE, D), DE ** -0.5, 0.1875, ((0, 32), (1, 2)))
    return dict(tokens=tokens, norm_gain=norm_gain, expert_ids=expert_ids, route_weights=route_weights, w_gate=w_gate, w_up=w_up, w_down=w_down)


def reference(tokens, norm_gain, expert_ids, route_weights, w_gate, w_up, w_down):
    values = tokens.astype(jnp.float32)
    scale = lax.rsqrt(lax.optimization_barrier(jnp.mean(values * values, axis=-1, keepdims=True)) + 1e-06)
    normed = (values * scale * norm_gain).astype(jnp.bfloat16)
    flat_ids = expert_ids.reshape(-1)
    flat_weights = route_weights.reshape(-1)
    total_rows = TOKENS // TOK_DEV * CAP

    def per_expert(carry, expert):
        chosen = flat_ids == expert
        count = jnp.sum(chosen.astype(jnp.int32))
        picks = jnp.nonzero(chosen, size=total_rows, fill_value=0)[0].astype(jnp.int32)
        live = jnp.arange(total_rows, dtype=jnp.int32) < count
        token_rows = picks // TOP_K
        rows = normed[token_rows]
        gate = jnp.dot(rows, w_gate[expert], preferred_element_type=jnp.float32)
        upper = jnp.dot(rows, w_up[expert], preferred_element_type=jnp.float32)
        hidden = (jax.nn.silu(gate) * upper).astype(jnp.bfloat16)
        result = jnp.dot(hidden, w_down[expert], preferred_element_type=jnp.float32).astype(jnp.bfloat16)
        result = lax.optimization_barrier(result).astype(jnp.float32)
        weight = jnp.where(live, flat_weights[picks], jnp.float32(0.0))
        carry = carry.at[token_rows].add(weight[:, None] * result)
        return (carry, None)
    start = jnp.zeros((TOKENS, D), jnp.float32)
    total, _ = lax.scan(per_expert, start, jnp.arange(EXPERTS, dtype=jnp.int32))
    return total.astype(jnp.bfloat16)
```

```python
import functools

import jax
import jax.numpy as jnp
from jax import lax
from jax.experimental import pallas as pl
from jax.experimental.pallas import tpu as pltpu
from jax.sharding import PartitionSpec as P

MESH = pl.DeviceIdType.MESH
CHUNK = 64
GROUP = 4


def prefix_sizes(tok, slots, ring):
    far = ring // 2
    sizes = [0] * (far + 2)
    for d in range(1, far + 1):
        rows = min(tok, slots * (far - d) + slots // 2)
        sizes[d] = -(-rows // 16) * 16
    return sizes


def chunks_of(rows):
    return [(lo, min(CHUNK, rows - lo)) for lo in range(0, rows, CHUNK)]


def moe_kernel(
    ring, slots, sizes, offs, shared,
    s_ref, meta_ref, ometa_ref, normed_ref, back_ref, wg_hbm, wu_hbm, wd_hbm,
    out_ref,
    held, meta_held, coming, final, contrib, x_ref, h_ref, o_ref, wj_ref,
    wg, wu, wd,
    d_send, d_recv, m_send, m_recv, r_send, r_recv, w_local, w_send, w_recv,
):
    z = lax.axis_index("ep")
    core = lax.axis_index("tp")
    far = ring // 2
    up = lax.rem(z + 1, ring)
    down = lax.rem(z + ring - 1, ring)
    onward = (up, down)
    home = (down, up)
    tok = s_ref.shape[1]
    pair = 2 * slots

    barrier = pltpu.get_barrier_semaphore()
    pl.semaphore_signal(barrier, inc=1, device_id={"ep": up}, device_id_type=MESH)
    pl.semaphore_signal(barrier, inc=1, device_id={"ep": down}, device_id_type=MESH)
    pl.semaphore_signal(barrier, inc=1, device_id={"tp": 1 - core}, device_id_type=MESH)
    pl.semaphore_wait(barrier, 3)

    def rows_out(way, d, lo, n):
        if d == 0:
            return s_ref.at[way, pl.ds(lo, n)]
        return held.at[way, pl.ds(offs[d] + lo, n)]

    def ring_copy(way, d, i, lo, n):
        return pltpu.make_async_remote_copy(
            src_ref=rows_out(way, d, lo, n),
            dst_ref=held.at[way, pl.ds(offs[d + 1] + lo, n)],
            send_sem=d_send.at[way, d],
            recv_sem=d_recv.at[way, d, i],
            device_id={"ep": onward[way]},
            device_id_type=MESH,
        )

    def meta_copy(way, d):
        return pltpu.make_async_remote_copy(
            src_ref=meta_ref.at[way] if d == 0 else meta_held.at[way, d - 1],
            dst_ref=meta_held.at[way, d],
            send_sem=m_send.at[way, d],
            recv_sem=m_recv.at[way, d],
            device_id={"ep": onward[way]},
            device_id_type=MESH,
        )

    def inbox(way, d, lo, n):
        if d == 0:
            return final.at[way, pl.ds(lo, n)]
        if d <= shared:
            return held.at[way, pl.ds(offs[d] + lo, n)]
        return coming.at[way, pl.ds(offs[d] - offs[shared + 1] + lo, n)]

    def home_copy(way, d, i, lo, n):
        return pltpu.make_async_remote_copy(
            src_ref=inbox(way, d, lo, n),
            dst_ref=inbox(way, d - 1, lo, n),
            send_sem=r_send.at[way, d - 1],
            recv_sem=r_recv.at[way, d - 1, i],
            device_id={"ep": home[way]},
            device_id_type=MESH,
        )

    def send_on(way, d):
        meta_copy(way, d).start()

    for way in (0, 1):
        meta_copy(way, 0).start()
    for i, (lo, n) in enumerate(chunks_of(sizes[1])):
        for way in (0, 1):
            ring_copy(way, 0, i, lo, n).start()

    weights = ((wg_hbm, wg), (wu_hbm, wu), (wd_hbm, wd))

    def own_weight(j):
        src, dst = weights[j]
        return pltpu.make_async_copy(src.at[0], dst.at[0], w_local.at[j])

    def peer_weight(j):
        src, dst = weights[j]
        return pltpu.make_async_remote_copy(
            src_ref=src.at[0], dst_ref=dst.at[1],
            send_sem=w_send.at[j], recv_sem=w_recv.at[j],
            device_id={"tp": 1 - core}, device_id_type=MESH,
        )

    for j in range(3):
        own_weight(j).start()
        peer_weight(j).start()

    slot_row = lax.broadcasted_iota(jnp.int32, (pair, 1), 0)
    base = (z * slots).astype(jnp.float32)
    first = jnp.where(slot_row < slots, base + slot_row.astype(jnp.float32), -2.0)
    second = jnp.where(slot_row >= slots, base + (slot_row - slots).astype(jnp.float32), -2.0)

    def matches(table, wanted):
        a = jnp.where(table[0:1, :] == wanted, 1.0, 0.0)
        b = jnp.where(table[1:2, :] == wanted, 1.0, 0.0)
        return a, b

    def picks(way, d):
        wanted = first if (way == 0 or d == far) else second
        return matches(meta_held[way, d - 1], wanted)

    def own_picks():
        return matches(ometa_ref[...], second)

    def weight_of(table, a, b):
        return jnp.sum(a * table[2:3, :] + b * table[3:4, :], axis=1, keepdims=True)

    def select(d):
        at = ((d - 1) % GROUP) * pair
        rows = sizes[d]
        total = jnp.zeros((pair, s_ref.shape[2]), jnp.float32)
        scale = jnp.zeros((pair, 1), jnp.float32)
        for way in (0, 1):
            a, b = picks(way, d)
            scale = scale + weight_of(meta_held[way, d - 1], a, b)
            one = (a + b).astype(jnp.bfloat16)[:, :rows]
            total = total + jnp.dot(
                one, held[way, pl.ds(offs[d], rows)], preferred_element_type=jnp.float32
            )
        if d == far:
            a, b = own_picks()
            scale = scale + weight_of(ometa_ref[...], a, b)
            total = total + jnp.dot(
                (a + b).astype(jnp.bfloat16), normed_ref[...], preferred_element_type=jnp.float32
            )
        x_ref[pl.ds(at, pair), :] = total.astype(jnp.bfloat16)
        wj_ref[pl.ds(at, pair), :] = jnp.broadcast_to(scale, (pair, wj_ref.shape[1]))

    def ffn(last):
        start = (last - GROUP) * pair
        rows = GROUP * pair
        half = wg.shape[2]
        tile = min(256, half)
        width = x_ref.shape[1]

        @pl.loop(0, 2)
        def _(part):
            for lo in range(0, half, tile):
                g = jnp.dot(x_ref[...], wg[part, :, lo:lo + tile], preferred_element_type=jnp.float32)
                u = jnp.dot(x_ref[...], wu[part, :, lo:lo + tile], preferred_element_type=jnp.float32)
                h_ref[part, :, lo:lo + tile] = ((g / (1.0 + jnp.exp(-g))) * u).astype(jnp.bfloat16)

        cols = min(512, width)

        @pl.loop(0, width // cols)
        def _(c):
            at = pl.ds(pl.multiple_of(c * cols, cols), cols)
            o = jnp.dot(h_ref[0], wd[0, :, at], preferred_element_type=jnp.float32)
            o = o + jnp.dot(h_ref[1], wd[1, :, at], preferred_element_type=jnp.float32)
            o_ref[pl.ds(start, rows), at] = (o * wj_ref[:, 0:1]).astype(jnp.bfloat16)

    for d in range(1, far + 1):
        if d >= 3:
            for way in (0, 1):
                ring_copy(way, d - 3, 0, 0, sizes[d - 2]).wait_send()
                meta_copy(way, d - 3).wait_send()
        for way in (0, 1):
            meta_copy(way, d - 1).wait_recv()
            if d < far:
                meta_copy(way, d).start()
        onwards = dict((lo, n) for lo, n in chunks_of(sizes[d + 1])) if d < far else {}
        for i, (lo, n) in enumerate(chunks_of(sizes[d])):
            for way in (0, 1):
                ring_copy(way, d - 1, i, lo, n).wait_recv()
                if lo in onwards:
                    ring_copy(way, d, i, lo, onwards[lo]).start()
        if d == GROUP:
            for j in range(3):
                own_weight(j).wait()
                peer_weight(j).wait()
        select(d)
        if d % GROUP == 0:
            ffn(d)
    for d in (far - 2, far - 1):
        for way in (0, 1):
            ring_copy(way, d, 0, 0, sizes[d + 1]).wait_send()
            meta_copy(way, d).wait_send()

    def contributions(way, d):
        a, b = picks(way, d)
        one = (a + b).astype(jnp.bfloat16)[:, :sizes[d]]
        got = lax.dot_general(
            one, o_ref[pl.ds((d - 1) * pair, pair), :], (((0,), (0,)), ((), ())),
            preferred_element_type=jnp.float32,
        )
        contrib[way, pl.ds(0, sizes[d])] = got.astype(jnp.bfloat16)

    for d in range(far, 0, -1):
        for way in (0, 1):
            contributions(way, d)
        arriving = dict((lo, n) for lo, n in chunks_of(sizes[d + 1])) if d < far else {}
        for i, (lo, n) in enumerate(chunks_of(sizes[d])):
            for way in (0, 1):
                m = arriving.get(lo, 0)
                if m:
                    home_copy(way, d + 1, i, lo, m).wait_recv()
                    was = inbox(way, d, lo, m)
                    was[...] = (
                        was[...].astype(jnp.float32)
                        + contrib[way, pl.ds(lo, m)].astype(jnp.float32)
                    ).astype(jnp.bfloat16)
                if m < n:
                    inbox(way, d, lo + m, n - m)[...] = contrib[way, pl.ds(lo + m, n - m)]
                home_copy(way, d, i, lo, n).start()
    for i, (lo, n) in enumerate(chunks_of(sizes[1])):
        for way in (0, 1):
            home_copy(way, 1, i, lo, n).wait_recv()

    a, b = own_picks()
    own = (a + b).astype(jnp.bfloat16)
    width = out_ref.shape[1]
    cols = min(512, width)

    @pl.loop(0, width // cols)
    def _(c):
        at = pl.ds(pl.multiple_of(c * cols, cols), cols)
        got = jnp.dot(back_ref[0], final[0, :, at], preferred_element_type=jnp.float32)
        got = got + jnp.dot(back_ref[1], final[1, :, at], preferred_element_type=jnp.float32)
        got = got + lax.dot_general(
            own, o_ref[pl.ds((far - 1) * pair, pair), at], (((0,), (0,)), ((), ())),
            preferred_element_type=jnp.float32,
        )
        out_ref[:, at] = got.astype(out_ref.dtype)

    for d in range(far, 0, -1):
        for way in (0, 1):
            home_copy(way, d, 0, 0, sizes[d]).wait_send()


def per_device(tokens, norm_gain, expert_ids, route_weights, w_gate, w_up, w_down):
    tok, width = tokens.shape
    top = expert_ids.shape[1]
    ring = lax.axis_size("ep")
    experts = w_gate.shape[0] * ring
    slots = 3 * tok * top // (2 * experts)
    far = ring // 2
    sizes = prefix_sizes(tok, slots, ring)
    offs, at = ([0] * (far + 2), 0)
    for d in range(1, far + 2):
        offs[d] = at
        at += sizes[d]
    total = at
    shared = far - 4
    half = w_gate.shape[2]
    pair = 2 * slots

    z = lax.axis_index("ep")
    values = tokens.astype(jnp.float32)
    scale = lax.rsqrt(jnp.mean(values * values, axis=-1, keepdims=True) + 1e-06)
    normed = (values * scale * norm_gain).astype(jnp.bfloat16)

    flat = expert_ids.reshape(-1)
    onehot = (flat[:, None] == jnp.arange(experts, dtype=jnp.int32)[None, :]).astype(jnp.bfloat16)
    count = tok * top
    earlier = (jnp.arange(count)[:, None] > jnp.arange(count)[None, :]).astype(jnp.bfloat16)
    before = jnp.dot(earlier, onehot, preferred_element_type=jnp.float32)
    slot = jnp.sum(before * onehot.astype(jnp.float32), axis=1).astype(jnp.int32).reshape(tok, top)
    target = (expert_ids * slots + slot).astype(jnp.float32)
    off = lax.rem(expert_ids - z + ring, ring)
    plus = ((off >= 1) & (off < far)) | ((off == far) & (slot < slots // 2))
    minus = (off > 0) & ~plus
    tables, backs, sorted_rows = ([], [], [])
    for mask, dist in ((plus, off), (minus, ring - off)):
        reach = jnp.max(jnp.where(mask, dist, 0), axis=1)
        ahead = (reach[None, :] > reach[:, None]) | (
            (reach[None, :] == reach[:, None])
            & (jnp.arange(tok)[None, :] < jnp.arange(tok)[:, None])
        )
        place = jnp.sum(ahead.astype(jnp.int32), axis=1)
        back = (place[:, None] == jnp.arange(tok)[None, :])
        table = jnp.concatenate(
            [jnp.where(mask, target, -1.0).T, route_weights.T, jnp.zeros((4, tok), jnp.float32)]
        )
        tables.append(jnp.dot(table, back.astype(jnp.float32), precision=lax.Precision.HIGHEST))
        back = back.astype(jnp.bfloat16)
        backs.append(back)
        sorted_rows.append(
            lax.dot_general(
                back, normed, (((0,), (0,)), ((), ())), preferred_element_type=jnp.float32
            ).astype(jnp.bfloat16)
        )
    own_table = jnp.concatenate(
        [jnp.where(off == 0, target, -1.0).T, route_weights.T, jnp.zeros((4, tok), jnp.float32)]
    )

    vm = pl.BlockSpec(memory_space=pltpu.VMEM)
    hbm = pl.BlockSpec(memory_space=pl.ANY)
    most = len(chunks_of(tok))
    bf16, f32 = jnp.bfloat16, jnp.float32
    call = pl.pallas_call(
        functools.partial(moe_kernel, ring, slots, sizes, offs, shared),
        out_shape=jax.ShapeDtypeStruct((tok, width), bf16),
        in_specs=[vm, vm, vm, vm, vm, hbm, hbm, hbm],
        out_specs=vm,
        scratch_shapes=[
            pltpu.VMEM((2, total, width), bf16),
            pltpu.VMEM((2, far, 8, tok), f32),
            pltpu.VMEM((2, total - offs[shared + 1], width), bf16),
            pltpu.VMEM((2, tok, width), bf16),
            pltpu.VMEM((2, tok, width), bf16),
            pltpu.VMEM((GROUP * pair, width), bf16),
            pltpu.VMEM((2, GROUP * pair, half), bf16),
            pltpu.VMEM((far * pair, width), bf16),
            pltpu.VMEM((GROUP * pair, 128), f32),
            pltpu.VMEM((2, width, half), bf16),
            pltpu.VMEM((2, width, half), bf16),
            pltpu.VMEM((2, half, width), bf16),
            pltpu.SemaphoreType.DMA((2, far)),
            pltpu.SemaphoreType.DMA((2, far, most)),
            pltpu.SemaphoreType.DMA((2, far)),
            pltpu.SemaphoreType.DMA((2, far)),
            pltpu.SemaphoreType.DMA((2, far)),
            pltpu.SemaphoreType.DMA((2, far, most)),
            pltpu.SemaphoreType.DMA((3,)),
            pltpu.SemaphoreType.DMA((3,)),
            pltpu.SemaphoreType.DMA((3,)),
        ],
        compiler_params=pltpu.CompilerParams(
            collective_id=0, has_side_effects=True, vmem_limit_bytes=67043328
        ),
        cost_estimate=pl.CostEstimate(
            flops=12 * tok * top * width * half, bytes_accessed=24 * width * half, transcendentals=0
        ),
    )
    return call(
        jnp.stack(sorted_rows), jnp.stack(tables), own_table, normed, jnp.stack(backs),
        w_gate, w_up, w_down,
    )


def solution(mesh):
    in_specs = (
        P(("grp", "ep", "tp"), None),
        P(),
        P(("grp", "ep", "tp"), None),
        P(("grp", "ep", "tp"), None),
        P("ep", None, "tp"),
        P("ep", None, "tp"),
        P("ep", "tp", None),
    )
    out_specs = P(("grp", "ep", "tp"), None)
    return jax.shard_map(
        per_device, mesh=mesh, in_specs=in_specs, out_specs=out_specs, check_vma=False
    )
```

```python
import functools

import jax
import jax.numpy as jnp
from jax import lax
from jax.experimental import pallas as pl
from jax.experimental.pallas import tpu as pltpu
from jax.sharding import PartitionSpec as P

MESH = pl.DeviceIdType.MESH
CHUNK = 64
REACH = 5


def prefix_sizes(tok, slots, far, reach):
    last = far - reach
    near = reach // 2
    sizes = [0] * (last + 2)
    for d in range(1, last + 1):
        rows = slots * (last - d) + slots // 2 + 2 * slots * max(0, near - d + 1)
        sizes[d] = -(-min(tok, rows) // 16) * 16
    return sizes


def chunks_of(rows):
    return [(lo, min(CHUNK, rows - lo)) for lo in range(0, rows, CHUNK)]


def block_plan(far, reach):
    near = reach // 2
    order = {0: [], 1: [], 2: []}
    for d in range(0, far - reach + 1):
        ways = (0,) if d == 0 else (0, 1)
        for way in ways:
            for copy in (0, 1, 2):
                main = d == 0 or copy == 1 + way
                if main or d <= near:
                    order[copy].append((way, d))
    places, at = ({}, 0)
    spans = {}
    for copy in (0, 1, 2):
        spans[copy] = at
        for key in order[copy]:
            places[(copy,) + key] = at
            at += 1
    return order, places, spans, at


def moe_kernel(
    ring, groups, slots, sizes, offs, shared,
    s_ref, meta_ref, sorted_own_ref, own_ref, back_ref, wg_hbm, wu_hbm, wd_hbm,
    out_ref,
    held, meta_held, coming, final, contrib, x_ref, h_ref, wj_ref,
    wg, wu, wd,
    d_send, d_recv, m_send, m_recv, r_send, r_recv,
    own_local, pair_send, pair_recv, far_send, far_recv, side_send, side_recv,
):
    g = lax.axis_index("grp")
    z = lax.axis_index("ep")
    core = lax.axis_index("tp")
    far = ring // 2
    last = far - REACH
    near = REACH // 2
    up = lax.rem(z + 1, ring)
    down = lax.rem(z + ring - 1, ring)
    far_up = lax.rem(z + REACH, ring)
    far_down = lax.rem(z + ring - REACH, ring)
    onward = (up, down)
    home = (down, up)
    block = -(-slots // 16) * 16
    order, places, spans, _ = block_plan(far, REACH)

    barrier = pltpu.get_barrier_semaphore()
    for there in (up, down, far_up, far_down):
        pl.semaphore_signal(barrier, inc=1, device_id={"ep": there}, device_id_type=MESH)
    pl.semaphore_signal(barrier, inc=1, device_id={"tp": 1 - core}, device_id_type=MESH)

    @pl.loop(1, groups)
    def _(j):
        pl.semaphore_signal(
            barrier, inc=1, device_id={"grp": lax.rem(g + j, groups)}, device_id_type=MESH
        )

    pl.semaphore_wait(barrier, 4 + groups)

    weights = ((wg_hbm, wg), (wu_hbm, wu), (wd_hbm, wd))

    def shard(j, which):
        rows = weights[j][0].shape[1] // groups
        return pl.ds(pl.multiple_of(which * rows, rows), rows)

    def far_copy(j, copy):
        src, dst = weights[j]
        return pltpu.make_async_remote_copy(
            src_ref=src.at[0, shard(j, g)],
            dst_ref=dst.at[copy, 0, shard(j, g)],
            send_sem=far_send.at[copy - 1, j],
            recv_sem=far_recv.at[copy - 1, j],
            device_id={"ep": far_down if copy == 1 else far_up},
            device_id_type=MESH,
        )

    def side_copy(j, copy, step, whose):
        ref = weights[j][1].at[copy, 0, shard(j, whose)]
        return pltpu.make_async_remote_copy(
            src_ref=ref, dst_ref=ref,
            send_sem=side_send.at[copy - 1, j, step],
            recv_sem=side_recv.at[copy - 1, j, step],
            device_id={"grp": lax.rem(g + step, groups)},
            device_id_type=MESH,
        )

    def pair_copy(j, copy):
        src, dst = weights[j]
        return pltpu.make_async_remote_copy(
            src_ref=src.at[0] if copy == 0 else dst.at[copy, 0],
            dst_ref=dst.at[copy, 1],
            send_sem=pair_send.at[copy, j],
            recv_sem=pair_recv.at[copy, j],
            device_id={"tp": 1 - core},
            device_id_type=MESH,
        )

    def own_weight(j):
        src, dst = weights[j]
        return pltpu.make_async_copy(src.at[0], dst.at[0, 0], own_local.at[j])

    def rows_out(way, d, lo, n):
        if d == 0:
            return s_ref.at[way, pl.ds(lo, n)]
        return held.at[way, pl.ds(offs[d] + lo, n)]

    def ring_copy(way, d, i, lo, n):
        return pltpu.make_async_remote_copy(
            src_ref=rows_out(way, d, lo, n),
            dst_ref=held.at[way, pl.ds(offs[d + 1] + lo, n)],
            send_sem=d_send.at[way, d],
            recv_sem=d_recv.at[way, d, i],
            device_id={"ep": onward[way]},
            device_id_type=MESH,
        )

    def meta_copy(way, d):
        return pltpu.make_async_remote_copy(
            src_ref=meta_ref.at[way] if d == 0 else meta_held.at[way, d - 1],
            dst_ref=meta_held.at[way, d],
            send_sem=m_send.at[way, d],
            recv_sem=m_recv.at[way, d],
            device_id={"ep": onward[way]},
            device_id_type=MESH,
        )

    def inbox(way, d, lo, n):
        if d == 0:
            return final.at[way, pl.ds(lo, n)]
        if d <= shared:
            return held.at[way, pl.ds(offs[d] + lo, n)]
        return coming.at[way, pl.ds(offs[d] - offs[shared + 1] + lo, n)]

    def home_copy(way, d, i, lo, n):
        return pltpu.make_async_remote_copy(
            src_ref=inbox(way, d, lo, n),
            dst_ref=inbox(way, d - 1, lo, n),
            send_sem=r_send.at[way, d - 1],
            recv_sem=r_recv.at[way, d - 1, i],
            device_id={"ep": home[way]},
            device_id_type=MESH,
        )

    for way in (0, 1):
        meta_copy(way, 0).start()
    for j in range(3):
        for copy in (1, 2):
            far_copy(j, copy).start()
    for i, (lo, n) in enumerate(chunks_of(sizes[1])):
        for way in (0, 1):
            ring_copy(way, 0, i, lo, n).start()
    for j in range(3):
        own_weight(j).start()
        pair_copy(j, 0).start()

    slot_row = lax.broadcasted_iota(jnp.int32, (block, 1), 0).astype(jnp.float32)
    wanted = tuple(
        jnp.where(slot_row < slots, (expert * slots).astype(jnp.float32) + slot_row, -2.0)
        for expert in (z, far_up, far_down)
    )

    def matches(table, copy):
        a = jnp.where(table[0:1, :] == wanted[copy], 1.0, 0.0)
        b = jnp.where(table[1:2, :] == wanted[copy], 1.0, 0.0)
        return a, b

    def table_of(way, d):
        return sorted_own_ref[...] if d == 0 else meta_held[way, d - 1]

    def select(way, d):
        rows = s_ref.shape[1] if d == 0 else sizes[d]
        table = table_of(way, d)
        for copy in (0, 1, 2):
            if (copy, way, d) not in places:
                continue
            at = pl.ds(places[(copy, way, d)] * block, block)
            a, b = matches(table, copy)
            scale = jnp.sum(a * table[2:3, :] + b * table[3:4, :], axis=1, keepdims=True)
            one = (a + b).astype(jnp.bfloat16)[:, :rows]
            source = s_ref[0] if d == 0 else held[way, pl.ds(offs[d], rows)]
            got = jnp.dot(one, source, preferred_element_type=jnp.float32)
            x_ref[at, :] = got.astype(jnp.bfloat16)
            wj_ref[at, :] = jnp.broadcast_to(scale, (block, wj_ref.shape[1]))

    def ffn(copy, lo_block, hi_block):
        start = (spans[copy] + lo_block) * block
        rows = (hi_block - lo_block) * block
        here = pl.ds(start, rows)
        half = wg.shape[3]
        tile = min(256, half)
        width = x_ref.shape[1]

        @pl.loop(0, 2)
        def _(part):
            for lo in range(0, half, tile):
                x = x_ref[here, :]
                a = jnp.dot(x, wg[copy, part, :, lo:lo + tile], preferred_element_type=jnp.float32)
                u = jnp.dot(x, wu[copy, part, :, lo:lo + tile], preferred_element_type=jnp.float32)
                h_ref[part, pl.ds(0, rows), lo:lo + tile] = (
                    (a / (1.0 + jnp.exp(-a))) * u
                ).astype(jnp.bfloat16)

        cols = min(512, width)

        @pl.loop(0, width // cols)
        def _(c):
            at = pl.ds(pl.multiple_of(c * cols, cols), cols)
            o = jnp.dot(h_ref[0, pl.ds(0, rows), :], wd[copy, 0, :, at], preferred_element_type=jnp.float32)
            o = o + jnp.dot(h_ref[1, pl.ds(0, rows), :], wd[copy, 1, :, at], preferred_element_type=jnp.float32)
            x_ref[here, at] = (o * wj_ref[here, 0:1]).astype(jnp.bfloat16)

    def upto(copy, d):
        return len([1 for key in order[copy] if key[1] <= d])

    def spread_weights():
        for j in range(3):
            for copy in (1, 2):
                far_copy(j, copy).wait_recv()

                @pl.loop(1, groups)
                def _(step):
                    side_copy(j, copy, step, g).start()

    def pair_weights():
        for j in range(3):
            for copy in (1, 2):

                @pl.loop(1, groups)
                def _(step):
                    side_copy(j, copy, step, lax.rem(g + groups - step, groups)).wait_recv()

                pair_copy(j, copy).start()

    def finish_weights():
        for j in range(3):
            for copy in (1, 2):
                pair_copy(j, copy).wait()
                far_copy(j, copy).wait_send()

                @pl.loop(1, groups)
                def _(step):
                    side_copy(j, copy, step, g).wait_send()

    select(0, 0)
    mid = (last + near + 1) // 2
    spread_weights()
    for d in range(1, last + 1):
        if d >= 3:
            for way in (0, 1):
                ring_copy(way, d - 3, 0, 0, sizes[d - 2]).wait_send()
                meta_copy(way, d - 3).wait_send()
        for way in (0, 1):
            meta_copy(way, d - 1).wait_recv()
            if d < last:
                meta_copy(way, d).start()
        onwards = dict((lo, n) for lo, n in chunks_of(sizes[d + 1])) if d < last else {}
        for i, (lo, n) in enumerate(chunks_of(sizes[d])):
            for way in (0, 1):
                ring_copy(way, d - 1, i, lo, n).wait_recv()
                if lo in onwards:
                    ring_copy(way, d, i, lo, onwards[lo]).start()
        for way in (0, 1):
            select(way, d)
        if d == near:
            for j in range(3):
                own_weight(j).wait()
                pair_copy(j, 0).wait()
            ffn(0, 0, upto(0, near))
            pair_weights()
        if d == mid:
            finish_weights()
            ffn(1, 0, upto(1, mid))
        if d == mid + 1:
            ffn(2, 0, upto(2, mid + 1))
    ffn(1, upto(1, mid), upto(1, last))
    ffn(2, upto(2, mid + 1), upto(2, last))
    for d in (last - 2, last - 1):
        for way in (0, 1):
            ring_copy(way, d, 0, 0, sizes[d + 1]).wait_send()
            meta_copy(way, d).wait_send()

    def gathered(table, rows, way, d, at):
        got = None
        for copy in (0, 1, 2):
            if (copy, way, d) not in places:
                continue
            a, b = matches(table, copy)
            one = (a + b).astype(jnp.bfloat16)[:, :rows]
            part = lax.dot_general(
                one, x_ref[pl.ds(places[(copy, way, d)] * block, block), at],
                (((0,), (0,)), ((), ())), preferred_element_type=jnp.float32,
            )
            got = part if got is None else got + part
        return got

    for d in range(last, 0, -1):
        for way in (0, 1):
            got = gathered(meta_held[way, d - 1], sizes[d], way, d, slice(None))
            contrib[way, pl.ds(0, sizes[d])] = got.astype(jnp.bfloat16)
        arriving = dict((lo, n) for lo, n in chunks_of(sizes[d + 1])) if d < last else {}
        for i, (lo, n) in enumerate(chunks_of(sizes[d])):
            for way in (0, 1):
                m = arriving.get(lo, 0)
                if m:
                    home_copy(way, d + 1, i, lo, m).wait_recv()
                    was = inbox(way, d, lo, m)
                    was[...] = (
                        was[...].astype(jnp.float32)
                        + contrib[way, pl.ds(lo, m)].astype(jnp.float32)
                    ).astype(jnp.bfloat16)
                if m < n:
                    inbox(way, d, lo + m, n - m)[...] = contrib[way, pl.ds(lo + m, n - m)]
                home_copy(way, d, i, lo, n).start()
    for i, (lo, n) in enumerate(chunks_of(sizes[1])):
        for way in (0, 1):
            home_copy(way, 1, i, lo, n).wait_recv()

    tok, width = out_ref.shape
    cols = min(512, width)

    @pl.loop(0, width // cols)
    def _(c):
        at = pl.ds(pl.multiple_of(c * cols, cols), cols)
        got = jnp.dot(back_ref[0], final[0, :, at], preferred_element_type=jnp.float32)
        got = got + jnp.dot(back_ref[1], final[1, :, at], preferred_element_type=jnp.float32)
        got = got + gathered(own_ref[...], tok, 0, 0, at)
        out_ref[:, at] = got.astype(out_ref.dtype)

    for d in range(last, 0, -1):
        for way in (0, 1):
            home_copy(way, d, 0, 0, sizes[d]).wait_send()


def per_device(tokens, norm_gain, expert_ids, route_weights, w_gate, w_up, w_down):
    tok, width = tokens.shape
    top = expert_ids.shape[1]
    ring = lax.axis_size("ep")
    groups = lax.axis_size("grp")
    experts = w_gate.shape[0] * ring
    slots = 3 * tok * top // (2 * experts)
    far = ring // 2
    last = far - REACH
    near = REACH // 2
    sizes = prefix_sizes(tok, slots, far, REACH)
    offs, at = ([0] * (last + 2), 0)
    for d in range(1, last + 2):
        offs[d] = at
        at += sizes[d]
    total = at
    shared = last - 4
    half = w_gate.shape[2]
    block = -(-slots // 16) * 16
    order, places, spans, blocks = block_plan(far, REACH)
    mid = (last + near + 1) // 2
    widest = max(
        len([1 for key in order[1] if key[1] <= mid]), len([1 for key in order[2] if key[1] <= mid + 1])
    )

    z = lax.axis_index("ep")
    values = tokens.astype(jnp.float32)
    scale = lax.rsqrt(jnp.mean(values * values, axis=-1, keepdims=True) + 1e-06)
    normed = (values * scale * norm_gain).astype(jnp.bfloat16)

    flat = expert_ids.reshape(-1)
    onehot = (flat[:, None] == jnp.arange(experts, dtype=jnp.int32)[None, :]).astype(jnp.bfloat16)
    count = tok * top
    earlier = (jnp.arange(count)[:, None] > jnp.arange(count)[None, :]).astype(jnp.bfloat16)
    before = jnp.dot(earlier, onehot, preferred_element_type=jnp.float32)
    slot = jnp.sum(before * onehot.astype(jnp.float32), axis=1).astype(jnp.int32).reshape(tok, top)
    target = (expert_ids * slots + slot).astype(jnp.float32)
    off = lax.rem(expert_ids - z + ring, ring)
    ahead_half = (off < far) | ((off == far) & (slot < slots // 2))
    signed = jnp.where(ahead_half, off, off - ring)
    host = jnp.where(
        jnp.abs(signed) <= near, signed, jnp.where(signed > 0, signed - REACH, signed + REACH)
    )
    extra = [route_weights.T, jnp.zeros((4, tok), jnp.float32)]
    own_table = jnp.concatenate([jnp.where(host == 0, target, -1.0).T] + extra)
    tables, backs, sorted_rows = ([], [], [])
    for dist in (host, -host):
        reach = jnp.max(jnp.maximum(dist, 0), axis=1)
        ahead = (reach[None, :] > reach[:, None]) | (
            (reach[None, :] == reach[:, None])
            & (jnp.arange(tok)[None, :] < jnp.arange(tok)[:, None])
        )
        place = jnp.sum(ahead.astype(jnp.int32), axis=1)
        back = (place[:, None] == jnp.arange(tok)[None, :])
        table = jnp.concatenate([jnp.where(dist > 0, target, -1.0).T] + extra)
        if not tables:
            table = jnp.concatenate([table, own_table])
        tables.append(jnp.dot(table, back.astype(jnp.float32), precision=lax.Precision.HIGHEST))
        back = back.astype(jnp.bfloat16)
        backs.append(back)
        sorted_rows.append(
            lax.dot_general(
                back, normed, (((0,), (0,)), ((), ())), preferred_element_type=jnp.float32
            ).astype(jnp.bfloat16)
        )
    sorted_own = tables[0][8:]
    tables[0] = tables[0][:8]

    vm = pl.BlockSpec(memory_space=pltpu.VMEM)
    hbm = pl.BlockSpec(memory_space=pl.ANY)
    most = len(chunks_of(tok))
    bf16, f32 = jnp.bfloat16, jnp.float32
    call = pl.pallas_call(
        functools.partial(moe_kernel, ring, groups, slots, sizes, offs, shared),
        out_shape=jax.ShapeDtypeStruct((tok, width), bf16),
        in_specs=[vm, vm, vm, vm, vm, hbm, hbm, hbm],
        out_specs=vm,
        scratch_shapes=[
            pltpu.VMEM((2, total, width), bf16),
            pltpu.VMEM((2, last, 8, tok), f32),
            pltpu.VMEM((2, total - offs[shared + 1], width), bf16),
            pltpu.VMEM((2, tok, width), bf16),
            pltpu.VMEM((2, tok, width), bf16),
            pltpu.VMEM((blocks * block, width), bf16),
            pltpu.VMEM((2, widest * block, half), bf16),
            pltpu.VMEM((blocks * block, 128), f32),
            pltpu.VMEM((3, 2, width, half), bf16),
            pltpu.VMEM((3, 2, width, half), bf16),
            pltpu.VMEM((3, 2, half, width), bf16),
            pltpu.SemaphoreType.DMA((2, last)),
            pltpu.SemaphoreType.DMA((2, last, most)),
            pltpu.SemaphoreType.DMA((2, last)),
            pltpu.SemaphoreType.DMA((2, last)),
            pltpu.SemaphoreType.DMA((2, last)),
            pltpu.SemaphoreType.DMA((2, last, most)),
            pltpu.SemaphoreType.DMA((3,)),
            pltpu.SemaphoreType.DMA((3, 3)),
            pltpu.SemaphoreType.DMA((3, 3)),
            pltpu.SemaphoreType.DMA((2, 3)),
            pltpu.SemaphoreType.DMA((2, 3)),
            pltpu.SemaphoreType.DMA((2, 3, groups)),
            pltpu.SemaphoreType.DMA((2, 3, groups)),
        ],
        compiler_params=pltpu.CompilerParams(
            collective_id=0, has_side_effects=True, vmem_limit_bytes=67043328
        ),
        cost_estimate=pl.CostEstimate(
            flops=12 * tok * top * width * half, bytes_accessed=24 * width * half, transcendentals=0
        ),
    )
    return call(
        jnp.stack(sorted_rows), jnp.stack(tables), sorted_own, own_table, jnp.stack(backs),
        w_gate, w_up, w_down,
    )


def solution(mesh):
    in_specs = (
        P(("grp", "ep", "tp"), None),
        P(),
        P(("grp", "ep", "tp"), None),
        P(("grp", "ep", "tp"), None),
        P("ep", None, "tp"),
        P("ep", None, "tp"),
        P("ep", "tp", None),
    )
    out_specs = P(("grp", "ep", "tp"), None)
    return jax.shard_map(
        per_device, mesh=mesh, in_specs=in_specs, out_specs=out_specs, check_vma=False
    )
```

```python
import functools

import jax
import jax.numpy as jnp
from jax import lax
from jax.experimental import pallas as pl
from jax.experimental.pallas import tpu as pltpu
from jax.sharding import PartitionSpec as P

MESH = pl.DeviceIdType.MESH
STEPS = (0, 16, 32, 64, 128, 192)
REACH = 5


def prefix_sizes(tok, slots, far, reach):
    last = far - reach
    near = reach // 2
    sizes = [0] * (last + 2)
    for d in range(1, last + 1):
        rows = slots * (last - d) + slots // 2 + 2 * slots * max(0, near - d + 1)
        sizes[d] = -(-min(tok, rows) // 8) * 8
    return sizes


def chunks_of(rows):
    starts = [lo for lo in STEPS if lo < rows]
    return list(zip(starts, [hi - lo for lo, hi in zip(starts, starts[1:] + [rows])]))


def block_plan(far, reach):
    near = reach // 2
    order = {0: [], 1: [], 2: []}
    for d in range(0, far - reach + 1):
        ways = (0,) if d == 0 else (0, 1)
        for way in ways:
            for copy in (0, 1, 2):
                main = d == 0 or copy == 1 + way
                if main or d <= near:
                    order[copy].append((way, d))
    places, at = ({}, 0)
    spans = {}
    for copy in (0, 1, 2):
        spans[copy] = at
        for key in order[copy]:
            places[(copy,) + key] = at
            at += 1
    return order, places, spans, at


def pass_ends(last, near):
    return (near + 2, last - 2, last)


def moe_kernel(
    ring, groups, slots, sizes, offs, shared,
    s_ref, meta_ref, sorted_own_ref, own_ref, back_ref, wg_hbm, wu_hbm, wd_hbm,
    out_ref,
    held, meta_held, coming, final, contrib, x_ref, h_ref, wj_ref,
    wg, wu, wd,
    d_send, d_recv, m_send, m_recv, r_send, r_recv,
    own_local, pair_send, pair_recv, far_send, far_recv, side_send, side_recv,
):
    g = lax.axis_index("grp")
    z = lax.axis_index("ep")
    core = lax.axis_index("tp")
    far = ring // 2
    last = far - REACH
    near = REACH // 2
    up = lax.rem(z + 1, ring)
    down = lax.rem(z + ring - 1, ring)
    far_up = lax.rem(z + REACH, ring)
    far_down = lax.rem(z + ring - REACH, ring)
    onward = (up, down)
    home = (down, up)
    block = -(-slots // 16) * 16
    order, places, spans, _ = block_plan(far, REACH)

    barrier = pltpu.get_barrier_semaphore()
    for there in (up, down, far_up, far_down):
        pl.semaphore_signal(barrier, inc=1, device_id={"ep": there}, device_id_type=MESH)
    pl.semaphore_signal(barrier, inc=1, device_id={"tp": 1 - core}, device_id_type=MESH)

    @pl.loop(1, groups)
    def _(j):
        pl.semaphore_signal(
            barrier, inc=1, device_id={"grp": lax.rem(g + j, groups)}, device_id_type=MESH
        )

    pl.semaphore_wait(barrier, 4 + groups)

    weights = ((wg_hbm, wg), (wu_hbm, wu), (wd_hbm, wd))

    def shard(j, which):
        rows = weights[j][0].shape[1] // groups
        return pl.ds(pl.multiple_of(which * rows, rows), rows)

    def far_copy(j, copy):
        src, dst = weights[j]
        return pltpu.make_async_remote_copy(
            src_ref=src.at[0, shard(j, g)],
            dst_ref=dst.at[copy, 0, shard(j, g)],
            send_sem=far_send.at[copy - 1, j],
            recv_sem=far_recv.at[copy - 1, j],
            device_id={"ep": far_down if copy == 1 else far_up},
            device_id_type=MESH,
        )

    def side_copy(j, copy, step, whose):
        ref = weights[j][1].at[copy, 0, shard(j, whose)]
        return pltpu.make_async_remote_copy(
            src_ref=ref, dst_ref=ref,
            send_sem=side_send.at[copy - 1, j, step],
            recv_sem=side_recv.at[copy - 1, j, step],
            device_id={"grp": lax.rem(g + step, groups)},
            device_id_type=MESH,
        )

    def pair_copy(j, copy):
        src, dst = weights[j]
        return pltpu.make_async_remote_copy(
            src_ref=src.at[0] if copy == 0 else dst.at[copy, 0],
            dst_ref=dst.at[copy, 1],
            send_sem=pair_send.at[copy, j],
            recv_sem=pair_recv.at[copy, j],
            device_id={"tp": 1 - core},
            device_id_type=MESH,
        )

    def own_weight(j):
        src, dst = weights[j]
        return pltpu.make_async_copy(src.at[0], dst.at[0, 0], own_local.at[j])

    def rows_out(way, d, lo, n):
        if d == 0:
            return s_ref.at[way, pl.ds(lo, n)]
        return held.at[way, pl.ds(offs[d] + lo, n)]

    def ring_copy(way, d, i, lo, n):
        return pltpu.make_async_remote_copy(
            src_ref=rows_out(way, d, lo, n),
            dst_ref=held.at[way, pl.ds(offs[d + 1] + lo, n)],
            send_sem=d_send.at[way, d],
            recv_sem=d_recv.at[way, d, i],
            device_id={"ep": onward[way]},
            device_id_type=MESH,
        )

    def meta_copy(way, d):
        return pltpu.make_async_remote_copy(
            src_ref=meta_ref.at[way] if d == 0 else meta_held.at[way, d - 1],
            dst_ref=meta_held.at[way, d],
            send_sem=m_send.at[way, d],
            recv_sem=m_recv.at[way, d],
            device_id={"ep": onward[way]},
            device_id_type=MESH,
        )

    def inbox(way, d, lo, n):
        if d == 0:
            return final.at[way, pl.ds(lo, n)]
        if d <= shared:
            return held.at[way, pl.ds(offs[d] + lo, n)]
        return coming.at[way, pl.ds(offs[d] - offs[shared + 1] + lo, n)]

    def home_copy(way, d, i, lo, n):
        return pltpu.make_async_remote_copy(
            src_ref=inbox(way, d, lo, n),
            dst_ref=inbox(way, d - 1, lo, n),
            send_sem=r_send.at[way, d - 1],
            recv_sem=r_recv.at[way, d - 1, i],
            device_id={"ep": home[way]},
            device_id_type=MESH,
        )

    for way in (0, 1):
        meta_copy(way, 0).start()
    for j in range(3):
        for copy in (1, 2):
            far_copy(j, copy).start()
    for i, (lo, n) in enumerate(chunks_of(sizes[1])):
        for way in (0, 1):
            ring_copy(way, 0, i, lo, n).start()
    for j in range(3):
        own_weight(j).start()
        pair_copy(j, 0).start()

    slot_row = lax.broadcasted_iota(jnp.int32, (block, 1), 0).astype(jnp.float32)
    wanted = tuple(
        jnp.where(slot_row < slots, (expert * slots).astype(jnp.float32) + slot_row, -2.0)
        for expert in (z, far_up, far_down)
    )

    def matches(table, copy):
        a = jnp.where(table[0:1, :] == wanted[copy], 1.0, 0.0)
        b = jnp.where(table[1:2, :] == wanted[copy], 1.0, 0.0)
        return a, b

    def table_of(way, d):
        return sorted_own_ref[...] if d == 0 else meta_held[way, d - 1]

    def select(way, d):
        rows = s_ref.shape[1] if d == 0 else sizes[d]
        table = table_of(way, d)
        for copy in (0, 1, 2):
            if (copy, way, d) not in places:
                continue
            at = pl.ds(places[(copy, way, d)] * block, block)
            a, b = matches(table, copy)
            scale = jnp.sum(a * table[2:3, :] + b * table[3:4, :], axis=1, keepdims=True)
            one = (a + b).astype(jnp.bfloat16)[:, :rows]
            source = s_ref[0] if d == 0 else held[way, pl.ds(offs[d], rows)]
            got = jnp.dot(one, source, preferred_element_type=jnp.float32)
            x_ref[at, :] = got.astype(jnp.bfloat16)
            wj_ref[at, :] = jnp.broadcast_to(scale, (block, wj_ref.shape[1]))

    def ffn(copy, lo_block, hi_block):
        start = (spans[copy] + lo_block) * block
        rows = (hi_block - lo_block) * block
        here = pl.ds(start, rows)
        half = wg.shape[3]
        tile = min(256, half)
        width = x_ref.shape[1]
        cols = min(512, width)

        def widen(part, lo):
            x = x_ref[here, :]
            a = jnp.dot(x, wg[copy, part, :, lo:lo + tile], preferred_element_type=jnp.float32)
            u = jnp.dot(x, wu[copy, part, :, lo:lo + tile], preferred_element_type=jnp.float32)
            h_ref[part, pl.ds(0, rows), lo:lo + tile] = (
                (a / (1.0 + jnp.exp(-a))) * u
            ).astype(jnp.bfloat16)

        def narrow(lo):
            at = slice(lo, lo + cols)
            o = jnp.dot(h_ref[0, pl.ds(0, rows), :], wd[copy, 0, :, at], preferred_element_type=jnp.float32)
            o = o + jnp.dot(h_ref[1, pl.ds(0, rows), :], wd[copy, 1, :, at], preferred_element_type=jnp.float32)
            x_ref[here, at] = (o * wj_ref[here, 0:1]).astype(jnp.bfloat16)

        return [
            functools.partial(widen, part, lo) for part in (0, 1) for lo in range(0, half, tile)
        ] + [functools.partial(narrow, lo) for lo in range(0, width, cols)]

    work = []

    def run(count):
        for piece in work[:count]:
            piece()
        del work[:count]

    def upto(copy, d):
        return len([1 for key in order[copy] if key[1] <= d])

    def spread_weights():
        for j in range(3):
            for copy in (1, 2):
                far_copy(j, copy).wait_recv()

                @pl.loop(1, groups)
                def _(step):
                    side_copy(j, copy, step, g).start()

    def pair_weights():
        for j in range(3):
            for copy in (1, 2):

                @pl.loop(1, groups)
                def _(step):
                    side_copy(j, copy, step, lax.rem(g + groups - step, groups)).wait_recv()

                pair_copy(j, copy).start()

    def finish_weights():
        for j in range(3):
            for copy in (1, 2):
                pair_copy(j, copy).wait()
                far_copy(j, copy).wait_send()

                @pl.loop(1, groups)
                def _(step):
                    side_copy(j, copy, step, g).wait_send()

    select(0, 0)
    cuts = pass_ends(last, near)
    spread_weights()
    for d in range(1, last + 1):
        if d >= 3:
            for way in (0, 1):
                ring_copy(way, d - 3, 0, 0, sizes[d - 2]).wait_send()
                meta_copy(way, d - 3).wait_send()
        for way in (0, 1):
            meta_copy(way, d - 1).wait_recv()
            if d < last:
                meta_copy(way, d).start()
        onwards = dict((lo, n) for lo, n in chunks_of(sizes[d + 1])) if d < last else {}
        for i, (lo, n) in enumerate(chunks_of(sizes[d])):
            for way in (0, 1):
                ring_copy(way, d - 1, i, lo, n).wait_recv()
                if lo in onwards:
                    ring_copy(way, d, i, lo, onwards[lo]).start()
            run(2)
        for way in (0, 1):
            select(way, d)
        if d == near:
            for j in range(3):
                own_weight(j).wait()
                pair_copy(j, 0).wait()
            work.extend(ffn(0, 0, upto(0, near)))
        if d == near + 1:
            pair_weights()
        if d in cuts:
            if d == cuts[0]:
                finish_weights()
            before = max([-1] + [cut for cut in cuts if cut < d])
            for copy in (1, 2):
                work.extend(ffn(copy, upto(copy, before), upto(copy, d)))
    run(len(work))
    for d in (last - 2, last - 1):
        for way in (0, 1):
            ring_copy(way, d, 0, 0, sizes[d + 1]).wait_send()
            meta_copy(way, d).wait_send()

    def gathered(table, rows, way, d, at):
        got = None
        for copy in (0, 1, 2):
            if (copy, way, d) not in places:
                continue
            a, b = matches(table, copy)
            one = (a + b).astype(jnp.bfloat16)[:, :rows]
            part = lax.dot_general(
                one, x_ref[pl.ds(places[(copy, way, d)] * block, block), at],
                (((0,), (0,)), ((), ())), preferred_element_type=jnp.float32,
            )
            got = part if got is None else got + part
        return got

    for d in range(last, 0, -1):
        for way in (0, 1):
            got = gathered(meta_held[way, d - 1], sizes[d], way, d, slice(None))
            contrib[way, pl.ds(0, sizes[d])] = got.astype(jnp.bfloat16)
        arriving = dict((lo, n) for lo, n in chunks_of(sizes[d + 1])) if d < last else {}
        for i, (lo, n) in enumerate(chunks_of(sizes[d])):
            for way in (0, 1):
                m = arriving.get(lo, 0)
                if m:
                    home_copy(way, d + 1, i, lo, m).wait_recv()
                    was = inbox(way, d, lo, m)
                    was[...] = (
                        was[...].astype(jnp.float32)
                        + contrib[way, pl.ds(lo, m)].astype(jnp.float32)
                    ).astype(jnp.bfloat16)
                if m < n:
                    inbox(way, d, lo + m, n - m)[...] = contrib[way, pl.ds(lo + m, n - m)]
                home_copy(way, d, i, lo, n).start()
    for i, (lo, n) in enumerate(chunks_of(sizes[1])):
        for way in (0, 1):
            home_copy(way, 1, i, lo, n).wait_recv()

    tok, width = out_ref.shape
    cols = min(512, width)

    @pl.loop(0, width // cols)
    def _(c):
        at = pl.ds(pl.multiple_of(c * cols, cols), cols)
        got = jnp.dot(back_ref[0], final[0, :, at], preferred_element_type=jnp.float32)
        got = got + jnp.dot(back_ref[1], final[1, :, at], preferred_element_type=jnp.float32)
        got = got + gathered(own_ref[...], tok, 0, 0, at)
        out_ref[:, at] = got.astype(out_ref.dtype)

    for d in range(last, 0, -1):
        for way in (0, 1):
            home_copy(way, d, 0, 0, sizes[d]).wait_send()


def per_device(tokens, norm_gain, expert_ids, route_weights, w_gate, w_up, w_down):
    tok, width = tokens.shape
    top = expert_ids.shape[1]
    ring = lax.axis_size("ep")
    groups = lax.axis_size("grp")
    experts = w_gate.shape[0] * ring
    slots = 3 * tok * top // (2 * experts)
    far = ring // 2
    last = far - REACH
    near = REACH // 2
    sizes = prefix_sizes(tok, slots, far, REACH)
    offs, at = ([0] * (last + 2), 0)
    for d in range(1, last + 2):
        offs[d] = at
        at += -(-sizes[d] // 16) * 16
    total = at
    shared = last - 4
    half = w_gate.shape[2]
    block = -(-slots // 16) * 16
    order, places, spans, blocks = block_plan(far, REACH)
    marks = [-1] + list(pass_ends(last, near))
    widest = max(
        len([1 for key in order[copy] if lo < key[1] <= hi])
        for copy in (0, 1, 2) for lo, hi in zip(marks, marks[1:])
    )

    z = lax.axis_index("ep")
    values = tokens.astype(jnp.float32)
    scale = lax.rsqrt(jnp.mean(values * values, axis=-1, keepdims=True) + 1e-06)
    normed = (values * scale * norm_gain).astype(jnp.bfloat16)

    flat = expert_ids.reshape(-1)
    onehot = (flat[:, None] == jnp.arange(experts, dtype=jnp.int32)[None, :]).astype(jnp.bfloat16)
    count = tok * top
    earlier = (jnp.arange(count)[:, None] > jnp.arange(count)[None, :]).astype(jnp.bfloat16)
    before = jnp.dot(earlier, onehot, preferred_element_type=jnp.float32)
    slot = jnp.sum(before * onehot.astype(jnp.float32), axis=1).astype(jnp.int32).reshape(tok, top)
    target = (expert_ids * slots + slot).astype(jnp.float32)
    off = lax.rem(expert_ids - z + ring, ring)
    ahead_half = (off < far) | ((off == far) & (slot < slots // 2))
    signed = jnp.where(ahead_half, off, off - ring)
    host = jnp.where(
        jnp.abs(signed) <= near, signed, jnp.where(signed > 0, signed - REACH, signed + REACH)
    )
    extra = [route_weights.T, jnp.zeros((4, tok), jnp.float32)]
    own_table = jnp.concatenate([jnp.where(host == 0, target, -1.0).T] + extra)
    tables, backs, sorted_rows = ([], [], [])
    for dist in (host, -host):
        reach = jnp.max(jnp.maximum(dist, 0), axis=1)
        ahead = (reach[None, :] > reach[:, None]) | (
            (reach[None, :] == reach[:, None])
            & (jnp.arange(tok)[None, :] < jnp.arange(tok)[:, None])
        )
        place = jnp.sum(ahead.astype(jnp.int32), axis=1)
        back = (place[:, None] == jnp.arange(tok)[None, :])
        table = jnp.concatenate([jnp.where(dist > 0, target, -1.0).T] + extra)
        if not tables:
            table = jnp.concatenate([table, own_table])
        tables.append(jnp.dot(table, back.astype(jnp.float32), precision=lax.Precision.HIGHEST))
        back = back.astype(jnp.bfloat16)
        backs.append(back)
        sorted_rows.append(
            lax.dot_general(
                back, normed, (((0,), (0,)), ((), ())), preferred_element_type=jnp.float32
            ).astype(jnp.bfloat16)
        )
    sorted_own = tables[0][8:]
    tables[0] = tables[0][:8]

    vm = pl.BlockSpec(memory_space=pltpu.VMEM)
    hbm = pl.BlockSpec(memory_space=pl.ANY)
    most = len(chunks_of(tok))
    bf16, f32 = jnp.bfloat16, jnp.float32
    call = pl.pallas_call(
        functools.partial(moe_kernel, ring, groups, slots, sizes, offs, shared),
        out_shape=jax.ShapeDtypeStruct((tok, width), bf16),
        in_specs=[vm, vm, vm, vm, vm, hbm, hbm, hbm],
        out_specs=vm,
        scratch_shapes=[
            pltpu.VMEM((2, total, width), bf16),
            pltpu.VMEM((2, last, 8, tok), f32),
            pltpu.VMEM((2, total - offs[shared + 1], width), bf16),
            pltpu.VMEM((2, tok, width), bf16),
            pltpu.VMEM((2, tok, width), bf16),
            pltpu.VMEM((blocks * block, width), bf16),
            pltpu.VMEM((2, widest * block, half), bf16),
            pltpu.VMEM((blocks * block, 128), f32),
            pltpu.VMEM((3, 2, width, half), bf16),
            pltpu.VMEM((3, 2, width, half), bf16),
            pltpu.VMEM((3, 2, half, width), bf16),
            pltpu.SemaphoreType.DMA((2, last)),
            pltpu.SemaphoreType.DMA((2, last, most)),
            pltpu.SemaphoreType.DMA((2, last)),
            pltpu.SemaphoreType.DMA((2, last)),
            pltpu.SemaphoreType.DMA((2, last)),
            pltpu.SemaphoreType.DMA((2, last, most)),
            pltpu.SemaphoreType.DMA((3,)),
            pltpu.SemaphoreType.DMA((3, 3)),
            pltpu.SemaphoreType.DMA((3, 3)),
            pltpu.SemaphoreType.DMA((2, 3)),
            pltpu.SemaphoreType.DMA((2, 3)),
            pltpu.SemaphoreType.DMA((2, 3, groups)),
            pltpu.SemaphoreType.DMA((2, 3, groups)),
        ],
        compiler_params=pltpu.CompilerParams(
            collective_id=0, has_side_effects=True, vmem_limit_bytes=67043328
        ),
        cost_estimate=pl.CostEstimate(
            flops=12 * tok * top * width * half, bytes_accessed=24 * width * half, transcendentals=0
        ),
    )
    return call(
        jnp.stack(sorted_rows), jnp.stack(tables), sorted_own, own_table, jnp.stack(backs),
        w_gate, w_up, w_down,
    )


def solution(mesh):
    in_specs = (
        P(("grp", "ep", "tp"), None),
        P(),
        P(("grp", "ep", "tp"), None),
        P(("grp", "ep", "tp"), None),
        P("ep", None, "tp"),
        P("ep", None, "tp"),
        P("ep", "tp", None),
    )
    out_specs = P(("grp", "ep", "tp"), None)
    return jax.shard_map(
        per_device, mesh=mesh, in_specs=in_specs, out_specs=out_specs, check_vma=False
    )
```

```python
import functools

import jax
import jax.numpy as jnp
from jax import lax
from jax.experimental import pallas as pl
from jax.experimental.pallas import tpu as pltpu
from jax.sharding import PartitionSpec as P

MESH = pl.DeviceIdType.MESH
STEPS = (0, 16, 32, 64, 128, 192)
REACH = 5


def prefix_sizes(tok, slots, far, reach):
    last = far - reach
    near = reach // 2
    sizes = [0] * (last + 2)
    for d in range(1, last + 1):
        rows = slots * (last - d) + slots // 2 + 2 * slots * max(0, near - d + 1)
        sizes[d] = -(-min(tok, rows) // 8) * 8
    return sizes


def chunks_of(rows):
    starts = [lo for lo in STEPS if lo < rows]
    return list(zip(starts, [hi - lo for lo, hi in zip(starts, starts[1:] + [rows])]))


def block_plan(far, reach):
    near = reach // 2
    order = {0: [], 1: [], 2: []}
    for d in range(0, far - reach + 1):
        ways = (0,) if d == 0 else (0, 1)
        for way in ways:
            for copy in (0, 1, 2):
                main = d == 0 or copy == 1 + way
                if main or d <= near:
                    order[copy].append((way, d))
    places, at = ({}, 0)
    spans = {}
    for copy in (0, 1, 2):
        spans[copy] = at
        for key in order[copy]:
            places[(copy,) + key] = at
            at += 1
    return order, places, spans, at


def pass_ends(last, near):
    return (near + 2, last - 2, last)


def moe_kernel(
    ring, groups, slots, sizes, offs, shared,
    tok_hbm, gain_ref, ids_ref, route_ref, wg_hbm, wu_hbm, wd_hbm,
    out_ref,
    s_ref, meta_ref, sorted_own_ref, own_ref, table_ref, back_ref, held, meta_held, coming, final, contrib, x_ref, h_ref, wj_ref,
    wg, wu, wd,
    d_send, d_recv, m_send, m_recv, r_send, r_recv,
    tok_local, own_local, pair_send, pair_recv, far_send, far_recv, side_send, side_recv,
):
    g = lax.axis_index("grp")
    z = lax.axis_index("ep")
    core = lax.axis_index("tp")
    far = ring // 2
    last = far - REACH
    near = REACH // 2
    up = lax.rem(z + 1, ring)
    down = lax.rem(z + ring - 1, ring)
    far_up = lax.rem(z + REACH, ring)
    far_down = lax.rem(z + ring - REACH, ring)
    onward = (up, down)
    home = (down, up)
    block = -(-slots // 16) * 16
    order, places, spans, _ = block_plan(far, REACH)

    tokens_in = pltpu.make_async_copy(tok_hbm, x_ref.at[pl.ds(0, out_ref.shape[0])], tok_local)
    tokens_in.start()
    barrier = pltpu.get_barrier_semaphore()
    for there in (up, down, far_up, far_down):
        pl.semaphore_signal(barrier, inc=1, device_id={"ep": there}, device_id_type=MESH)
    pl.semaphore_signal(barrier, inc=1, device_id={"tp": 1 - core}, device_id_type=MESH)

    @pl.loop(1, groups)
    def _(j):
        pl.semaphore_signal(
            barrier, inc=1, device_id={"grp": lax.rem(g + j, groups)}, device_id_type=MESH
        )

    pl.semaphore_wait(barrier, 4 + groups)

    weights = ((wg_hbm, wg), (wu_hbm, wu), (wd_hbm, wd))

    def shard(j, which):
        rows = weights[j][0].shape[1] // groups
        return pl.ds(pl.multiple_of(which * rows, rows), rows)

    def far_copy(j, copy):
        src, dst = weights[j]
        return pltpu.make_async_remote_copy(
            src_ref=src.at[0, shard(j, g)],
            dst_ref=dst.at[copy, 0, shard(j, g)],
            send_sem=far_send.at[copy - 1, j],
            recv_sem=far_recv.at[copy - 1, j],
            device_id={"ep": far_down if copy == 1 else far_up},
            device_id_type=MESH,
        )

    def side_copy(j, copy, step, whose):
        ref = weights[j][1].at[copy, 0, shard(j, whose)]
        return pltpu.make_async_remote_copy(
            src_ref=ref, dst_ref=ref,
            send_sem=side_send.at[copy - 1, j, step],
            recv_sem=side_recv.at[copy - 1, j, step],
            device_id={"grp": lax.rem(g + step, groups)},
            device_id_type=MESH,
        )

    def pair_copy(j, copy):
        src, dst = weights[j]
        return pltpu.make_async_remote_copy(
            src_ref=src.at[0] if copy == 0 else dst.at[copy, 0],
            dst_ref=dst.at[copy, 1],
            send_sem=pair_send.at[copy, j],
            recv_sem=pair_recv.at[copy, j],
            device_id={"tp": 1 - core},
            device_id_type=MESH,
        )

    def own_weight(j):
        src, dst = weights[j]
        return pltpu.make_async_copy(src.at[0], dst.at[0, 0], own_local.at[j])

    def rows_out(way, d, lo, n):
        if d == 0:
            return s_ref.at[way, pl.ds(lo, n)]
        return held.at[way, pl.ds(offs[d] + lo, n)]

    def ring_copy(way, d, i, lo, n):
        return pltpu.make_async_remote_copy(
            src_ref=rows_out(way, d, lo, n),
            dst_ref=held.at[way, pl.ds(offs[d + 1] + lo, n)],
            send_sem=d_send.at[way, d],
            recv_sem=d_recv.at[way, d, i],
            device_id={"ep": onward[way]},
            device_id_type=MESH,
        )

    def meta_copy(way, d):
        return pltpu.make_async_remote_copy(
            src_ref=meta_ref.at[way] if d == 0 else meta_held.at[way, d - 1],
            dst_ref=meta_held.at[way, d],
            send_sem=m_send.at[way, d],
            recv_sem=m_recv.at[way, d],
            device_id={"ep": onward[way]},
            device_id_type=MESH,
        )

    def inbox(way, d, lo, n):
        if d == 0:
            return final.at[way, pl.ds(lo, n)]
        if d <= shared:
            return held.at[way, pl.ds(offs[d] + lo, n)]
        return coming.at[way, pl.ds(offs[d] - offs[shared + 1] + lo, n)]

    def home_copy(way, d, i, lo, n):
        return pltpu.make_async_remote_copy(
            src_ref=inbox(way, d, lo, n),
            dst_ref=inbox(way, d - 1, lo, n),
            send_sem=r_send.at[way, d - 1],
            recv_sem=r_recv.at[way, d - 1, i],
            device_id={"ep": home[way]},
            device_id_type=MESH,
        )

    for j in range(3):
        for copy in (1, 2):
            far_copy(j, copy).start()
    for j in range(3):
        own_weight(j).start()
        pair_copy(j, 0).start()

    tok = out_ref.shape[0]
    tokens_in.wait()
    step = min(64, tok)

    @pl.loop(0, tok // step)
    def _(i):
        at = pl.ds(pl.multiple_of(i * step, step), step)
        values = x_ref[at, :].astype(jnp.float32)
        scale = lax.rsqrt(jnp.mean(values * values, axis=-1, keepdims=True) + 1e-06)
        contrib[0, at, :] = (values * scale * gain_ref[...]).astype(jnp.bfloat16)

    down_at = lax.broadcasted_iota(jnp.int32, (tok, tok), 0)
    across_at = lax.broadcasted_iota(jnp.int32, (tok, tok), 1)
    before_it = down_at < across_at

    def column(row):
        return jnp.sum(jnp.where(down_at == across_at, row, 0.0), axis=1, keepdims=True)

    def count_down(test):
        return jnp.sum(jnp.where(test, 1.0, 0.0), axis=0, keepdims=True)

    ids = [ids_ref[k:k + 1, :].astype(jnp.float32) for k in (0, 1)]
    routes = [route_ref[k:k + 1, :] for k in (0, 1)]
    id_columns = [column(row) for row in ids]
    hosts, targets = ([], [])
    for k in (0, 1):
        named = (id_columns[0] == ids[k]) | (id_columns[1] == ids[k])
        slot = count_down(named & before_it)
        targets.append(ids[k] * slots + slot)
        off = ids[k] - z.astype(jnp.float32)
        off = jnp.where(off < 0.0, off + ring, off)
        ahead_half = (off < far) | ((off == far) & (slot < slots // 2))
        signed = jnp.where(ahead_half, off, off - ring)
        hosts.append(
            jnp.where(
                jnp.abs(signed) <= near, signed,
                jnp.where(signed > 0.0, signed - REACH, signed + REACH),
            )
        )
    own_ref[...] = jnp.zeros_like(own_ref)
    for k in (0, 1):
        own_ref[k:k + 1, :] = jnp.where(hosts[k] == 0.0, targets[k], -1.0)
        own_ref[2 + k:3 + k, :] = routes[k]
    for way in (0, 1):
        dist = [host if way == 0 else -host for host in hosts]
        reach = jnp.maximum(jnp.maximum(dist[0], dist[1]), 0.0)
        reach_column = column(reach)
        place = count_down((reach_column > reach) | ((reach_column == reach) & before_it))
        back = jnp.where(column(place) == across_at.astype(jnp.float32), 1.0, 0.0)
        back_ref[way] = back.astype(jnp.bfloat16)
        table = table_ref
        table[...] = jnp.zeros_like(own_ref)
        for k in (0, 1):
            table[k:k + 1, :] = jnp.where(dist[k] > 0.0, targets[k], -1.0)
            table[2 + k:3 + k, :] = routes[k]
        meta_ref[way] = jnp.dot(
            table[...], back, precision=lax.Precision.HIGHEST, preferred_element_type=jnp.float32
        )
        if way == 0:
            sorted_own_ref[...] = jnp.dot(
                own_ref[...], back, precision=lax.Precision.HIGHEST, preferred_element_type=jnp.float32
            )
        pick = jnp.where(place == down_at.astype(jnp.float32), 1.0, 0.0).astype(jnp.bfloat16)
        s_ref[way] = jnp.dot(
            pick, contrib[0], preferred_element_type=jnp.float32
        ).astype(jnp.bfloat16)
        meta_copy(way, 0).start()
        for i, (lo, n) in enumerate(chunks_of(sizes[1])):
            ring_copy(way, 0, i, lo, n).start()

    slot_row = lax.broadcasted_iota(jnp.int32, (block, 1), 0).astype(jnp.float32)
    wanted = tuple(
        jnp.where(slot_row < slots, (expert * slots).astype(jnp.float32) + slot_row, -2.0)
        for expert in (z, far_up, far_down)
    )

    def matches(table, copy):
        a = jnp.where(table[0:1, :] == wanted[copy], 1.0, 0.0)
        b = jnp.where(table[1:2, :] == wanted[copy], 1.0, 0.0)
        return a, b

    def table_of(way, d):
        return sorted_own_ref[...] if d == 0 else meta_held[way, d - 1]

    def select(way, d):
        rows = s_ref.shape[1] if d == 0 else sizes[d]
        table = table_of(way, d)
        for copy in (0, 1, 2):
            if (copy, way, d) not in places:
                continue
            at = pl.ds(places[(copy, way, d)] * block, block)
            a, b = matches(table, copy)
            scale = jnp.sum(a * table[2:3, :] + b * table[3:4, :], axis=1, keepdims=True)
            one = (a + b).astype(jnp.bfloat16)[:, :rows]
            source = s_ref[0] if d == 0 else held[way, pl.ds(offs[d], rows)]
            got = jnp.dot(one, source, preferred_element_type=jnp.float32)
            x_ref[at, :] = got.astype(jnp.bfloat16)
            wj_ref[at, :] = jnp.broadcast_to(scale, (block, wj_ref.shape[1]))

    def ffn(copy, lo_block, hi_block):
        start = (spans[copy] + lo_block) * block
        rows = (hi_block - lo_block) * block
        here = pl.ds(start, rows)
        half = wg.shape[3]
        tile = min(256, half)
        width = x_ref.shape[1]
        cols = min(512, width)

        def widen(part, lo):
            x = x_ref[here, :]
            a = jnp.dot(x, wg[copy, part, :, lo:lo + tile], preferred_element_type=jnp.float32)
            u = jnp.dot(x, wu[copy, part, :, lo:lo + tile], preferred_element_type=jnp.float32)
            h_ref[part, pl.ds(0, rows), lo:lo + tile] = (
                (a / (1.0 + jnp.exp(-a))) * u
            ).astype(jnp.bfloat16)

        def narrow(lo):
            at = slice(lo, lo + cols)
            o = jnp.dot(h_ref[0, pl.ds(0, rows), :], wd[copy, 0, :, at], preferred_element_type=jnp.float32)
            o = o + jnp.dot(h_ref[1, pl.ds(0, rows), :], wd[copy, 1, :, at], preferred_element_type=jnp.float32)
            x_ref[here, at] = (o * wj_ref[here, 0:1]).astype(jnp.bfloat16)

        return [
            functools.partial(widen, part, lo) for part in (0, 1) for lo in range(0, half, tile)
        ] + [functools.partial(narrow, lo) for lo in range(0, width, cols)]

    work = []

    def run(count):
        for piece in work[:count]:
            piece()
        del work[:count]

    def upto(copy, d):
        return len([1 for key in order[copy] if key[1] <= d])

    def spread_weights():
        for j in range(3):
            for copy in (1, 2):
                far_copy(j, copy).wait_recv()

                @pl.loop(1, groups)
                def _(step):
                    side_copy(j, copy, step, g).start()

    def pair_weights():
        for j in range(3):
            for copy in (1, 2):

                @pl.loop(1, groups)
                def _(step):
                    side_copy(j, copy, step, lax.rem(g + groups - step, groups)).wait_recv()

                pair_copy(j, copy).start()

    def finish_weights():
        for j in range(3):
            for copy in (1, 2):
                pair_copy(j, copy).wait()
                far_copy(j, copy).wait_send()

                @pl.loop(1, groups)
                def _(step):
                    side_copy(j, copy, step, g).wait_send()

    select(0, 0)
    cuts = pass_ends(last, near)
    spread_weights()
    for d in range(1, last + 1):
        if d >= 3:
            for way in (0, 1):
                ring_copy(way, d - 3, 0, 0, sizes[d - 2]).wait_send()
                meta_copy(way, d - 3).wait_send()
        for way in (0, 1):
            meta_copy(way, d - 1).wait_recv()
            if d < last:
                meta_copy(way, d).start()
        onwards = dict((lo, n) for lo, n in chunks_of(sizes[d + 1])) if d < last else {}
        for i, (lo, n) in enumerate(chunks_of(sizes[d])):
            for way in (0, 1):
                ring_copy(way, d - 1, i, lo, n).wait_recv()
                if lo in onwards:
                    ring_copy(way, d, i, lo, onwards[lo]).start()
            run(2)
        for way in (0, 1):
            select(way, d)
        if d == near:
            for j in range(3):
                own_weight(j).wait()
                pair_copy(j, 0).wait()
            work.extend(ffn(0, 0, upto(0, near)))
        if d == near + 1:
            pair_weights()
        if d in cuts:
            if d == cuts[0]:
                finish_weights()
            before = max([-1] + [cut for cut in cuts if cut < d])
            for copy in (1, 2):
                work.extend(ffn(copy, upto(copy, before), upto(copy, d)))
    run(len(work))
    for d in (last - 2, last - 1):
        for way in (0, 1):
            ring_copy(way, d, 0, 0, sizes[d + 1]).wait_send()
            meta_copy(way, d).wait_send()

    def gathered(table, rows, way, d, at):
        got = None
        for copy in (0, 1, 2):
            if (copy, way, d) not in places:
                continue
            a, b = matches(table, copy)
            one = (a + b).astype(jnp.bfloat16)[:, :rows]
            part = lax.dot_general(
                one, x_ref[pl.ds(places[(copy, way, d)] * block, block), at],
                (((0,), (0,)), ((), ())), preferred_element_type=jnp.float32,
            )
            got = part if got is None else got + part
        return got

    for d in range(last, 0, -1):
        for way in (0, 1):
            got = gathered(meta_held[way, d - 1], sizes[d], way, d, slice(None))
            contrib[way, pl.ds(0, sizes[d])] = got.astype(jnp.bfloat16)
        arriving = dict((lo, n) for lo, n in chunks_of(sizes[d + 1])) if d < last else {}
        for i, (lo, n) in enumerate(chunks_of(sizes[d])):
            for way in (0, 1):
                m = arriving.get(lo, 0)
                if m:
                    home_copy(way, d + 1, i, lo, m).wait_recv()
                    was = inbox(way, d, lo, m)
                    was[...] = (
                        was[...].astype(jnp.float32)
                        + contrib[way, pl.ds(lo, m)].astype(jnp.float32)
                    ).astype(jnp.bfloat16)
                if m < n:
                    inbox(way, d, lo + m, n - m)[...] = contrib[way, pl.ds(lo + m, n - m)]
                home_copy(way, d, i, lo, n).start()
    for i, (lo, n) in enumerate(chunks_of(sizes[1])):
        for way in (0, 1):
            home_copy(way, 1, i, lo, n).wait_recv()

    tok, width = out_ref.shape
    cols = min(512, width)

    @pl.loop(0, width // cols)
    def _(c):
        at = pl.ds(pl.multiple_of(c * cols, cols), cols)
        got = jnp.dot(back_ref[0], final[0, :, at], preferred_element_type=jnp.float32)
        got = got + jnp.dot(back_ref[1], final[1, :, at], preferred_element_type=jnp.float32)
        got = got + gathered(own_ref[...], tok, 0, 0, at)
        out_ref[:, at] = got.astype(out_ref.dtype)

    for d in range(last, 0, -1):
        for way in (0, 1):
            home_copy(way, d, 0, 0, sizes[d]).wait_send()


def per_device(tokens, norm_gain, expert_ids, route_weights, w_gate, w_up, w_down):
    tok, width = tokens.shape
    top = expert_ids.shape[1]
    ring = lax.axis_size("ep")
    groups = lax.axis_size("grp")
    experts = w_gate.shape[0] * ring
    slots = 3 * tok * top // (2 * experts)
    far = ring // 2
    last = far - REACH
    near = REACH // 2
    sizes = prefix_sizes(tok, slots, far, REACH)
    offs, at = ([0] * (last + 2), 0)
    for d in range(1, last + 2):
        offs[d] = at
        at += -(-sizes[d] // 16) * 16
    total = at
    shared = last - 4
    half = w_gate.shape[2]
    block = -(-slots // 16) * 16
    order, places, spans, blocks = block_plan(far, REACH)
    marks = [-1] + list(pass_ends(last, near))
    widest = max(
        len([1 for key in order[copy] if lo < key[1] <= hi])
        for copy in (0, 1, 2) for lo, hi in zip(marks, marks[1:])
    )

    vm = pl.BlockSpec(memory_space=pltpu.VMEM)
    hbm = pl.BlockSpec(memory_space=pl.ANY)
    most = len(chunks_of(tok))
    bf16, f32 = jnp.bfloat16, jnp.float32
    call = pl.pallas_call(
        functools.partial(moe_kernel, ring, groups, slots, sizes, offs, shared),
        out_shape=jax.ShapeDtypeStruct((tok, width), bf16),
        in_specs=[hbm, vm, vm, vm, hbm, hbm, hbm],
        out_specs=vm,
        scratch_shapes=[
            pltpu.VMEM((2, tok, width), bf16),
            pltpu.VMEM((2, 8, tok), f32),
            pltpu.VMEM((8, tok), f32),
            pltpu.VMEM((8, tok), f32),
            pltpu.VMEM((8, tok), f32),
            pltpu.VMEM((2, tok, tok), bf16),
            pltpu.VMEM((2, total, width), bf16),
            pltpu.VMEM((2, last, 8, tok), f32),
            pltpu.VMEM((2, total - offs[shared + 1], width), bf16),
            pltpu.VMEM((2, tok, width), bf16),
            pltpu.VMEM((2, tok, width), bf16),
            pltpu.VMEM((blocks * block, width), bf16),
            pltpu.VMEM((2, widest * block, half), bf16),
            pltpu.VMEM((blocks * block, 128), f32),
            pltpu.VMEM((3, 2, width, half), bf16),
            pltpu.VMEM((3, 2, width, half), bf16),
            pltpu.VMEM((3, 2, half, width), bf16),
            pltpu.SemaphoreType.DMA((2, last)),
            pltpu.SemaphoreType.DMA((2, last, most)),
            pltpu.SemaphoreType.DMA((2, last)),
            pltpu.SemaphoreType.DMA((2, last)),
            pltpu.SemaphoreType.DMA((2, last)),
            pltpu.SemaphoreType.DMA((2, last, most)),
            pltpu.SemaphoreType.DMA,
            pltpu.SemaphoreType.DMA((3,)),
            pltpu.SemaphoreType.DMA((3, 3)),
            pltpu.SemaphoreType.DMA((3, 3)),
            pltpu.SemaphoreType.DMA((2, 3)),
            pltpu.SemaphoreType.DMA((2, 3)),
            pltpu.SemaphoreType.DMA((2, 3, groups)),
            pltpu.SemaphoreType.DMA((2, 3, groups)),
        ],
        compiler_params=pltpu.CompilerParams(
            collective_id=0, has_side_effects=True, vmem_limit_bytes=67043328
        ),
        cost_estimate=pl.CostEstimate(
            flops=12 * tok * top * width * half, bytes_accessed=24 * width * half, transcendentals=0
        ),
    )
    return call(
        tokens, norm_gain.reshape(1, width), expert_ids.T, route_weights.T,
        w_gate, w_up, w_down,
    )


def solution(mesh):
    in_specs = (
        P(("grp", "ep", "tp"), None),
        P(),
        P(("grp", "ep", "tp"), None),
        P(("grp", "ep", "tp"), None),
        P("ep", None, "tp"),
        P("ep", None, "tp"),
        P("ep", "tp", None),
    )
    out_specs = P(("grp", "ep", "tp"), None)
    return jax.shard_map(
        per_device, mesh=mesh, in_specs=in_specs, out_specs=out_specs, check_vma=False
    )
```

```python
import functools

import jax
import jax.numpy as jnp
from jax import lax
from jax.experimental import pallas as pl
from jax.experimental.pallas import tpu as pltpu
from jax.sharding import PartitionSpec as P

MESH = pl.DeviceIdType.MESH
STEPS = (0, 16, 32, 64, 128, 192)
REACH = 5


def opposite_split(slots):
    return -(-slots // 16) * 8


def prefix_sizes(tok, slots, far, reach, way):
    first = opposite_split(slots)
    at_far = first if way == 0 else slots - first
    last = far - reach
    near = reach // 2
    sizes = [0] * (last + 2)
    for d in range(1, last + 1):
        rows = slots * (last - d) + at_far + 2 * slots * max(0, near - d + 1)
        sizes[d] = -(-min(tok, rows) // 8) * 8
    return sizes


def chunks_of(rows):
    starts = [lo for lo in STEPS if lo < rows]
    return list(zip(starts, [hi - lo for lo, hi in zip(starts, starts[1:] + [rows])]))


def block_plan(far, reach):
    near = reach // 2
    order = {0: [], 1: [], 2: []}
    for d in range(0, far - reach + 1):
        ways = (0,) if d == 0 else (0, 1)
        for way in ways:
            for copy in (0, 1, 2):
                main = d == 0 or copy == 1 + way
                if main or d <= near:
                    order[copy].append((way, d))
    places, at = ({}, 0)
    spans = {}
    for copy in (0, 1, 2):
        spans[copy] = at
        for key in order[copy]:
            places[(copy,) + key] = at
            at += 1
    return order, places, spans, at


def pass_ends(last, near):
    return (near + 2, last - 3, last)


def moe_kernel(
    ring, groups, slots, sizes, offs, shared,
    tok_hbm, gain_ref, ids_ref, route_ref, wg_hbm, wu_hbm, wd_hbm,
    out_ref,
    s_ref, meta_ref, sorted_own_ref, own_ref, table_ref, back_ref, held, meta_held, coming, final, contrib, x_ref, h_ref, wj_ref,
    wg, wu, wd,
    d_send, d_recv, m_send, m_recv, r_send, r_recv,
    tok_local, own_local, pair_send, pair_recv, far_send, far_recv, side_send, side_recv,
):
    g = lax.axis_index("grp")
    z = lax.axis_index("ep")
    core = lax.axis_index("tp")
    far = ring // 2
    last = far - REACH
    near = REACH // 2
    turn = 1 - 2 * core
    up = lax.rem(z + ring + turn, ring)
    down = lax.rem(z + ring - turn, ring)
    far_up = lax.rem(z + ring + turn * REACH, ring)
    far_down = lax.rem(z + ring - turn * REACH, ring)
    onward = (up, down)
    home = (down, up)
    block = -(-slots // 16) * 16
    order, places, spans, _ = block_plan(far, REACH)

    tokens_in = pltpu.make_async_copy(tok_hbm, x_ref.at[pl.ds(0, out_ref.shape[0])], tok_local)
    tokens_in.start()
    barrier = pltpu.get_barrier_semaphore()
    for there in (up, down, far_up, far_down):
        pl.semaphore_signal(barrier, inc=1, device_id={"ep": there}, device_id_type=MESH)
    pl.semaphore_signal(barrier, inc=1, device_id={"tp": 1 - core}, device_id_type=MESH)

    @pl.loop(1, groups)
    def _(j):
        pl.semaphore_signal(
            barrier, inc=1, device_id={"grp": lax.rem(g + j, groups)}, device_id_type=MESH
        )

    pl.semaphore_wait(barrier, 4 + groups)

    weights = ((wg_hbm, wg), (wu_hbm, wu), (wd_hbm, wd))

    def shard(j, which):
        rows = weights[j][0].shape[1] // groups
        return pl.ds(pl.multiple_of(which * rows, rows), rows)

    def far_copy(j, copy):
        src, dst = weights[j]
        return pltpu.make_async_remote_copy(
            src_ref=src.at[0, shard(j, g)],
            dst_ref=dst.at[copy, 0, shard(j, g)],
            send_sem=far_send.at[copy - 1, j],
            recv_sem=far_recv.at[copy - 1, j],
            device_id={"ep": far_down if copy == 1 else far_up},
            device_id_type=MESH,
        )

    def side_copy(j, copy, step, whose):
        ref = weights[j][1].at[copy, 0, shard(j, whose)]
        return pltpu.make_async_remote_copy(
            src_ref=ref, dst_ref=ref,
            send_sem=side_send.at[copy - 1, j, step],
            recv_sem=side_recv.at[copy - 1, j, step],
            device_id={"grp": lax.rem(g + step, groups)},
            device_id_type=MESH,
        )

    def pair_copy(j, copy):
        src, dst = weights[j]
        there = (0, 2, 1)[copy]
        return pltpu.make_async_remote_copy(
            src_ref=src.at[0] if copy == 0 else dst.at[copy, 0],
            dst_ref=dst.at[there, 1],
            send_sem=pair_send.at[copy, j],
            recv_sem=pair_recv.at[there, j],
            device_id={"tp": 1 - core},
            device_id_type=MESH,
        )

    def own_weight(j):
        src, dst = weights[j]
        return pltpu.make_async_copy(src.at[0], dst.at[0, 0], own_local.at[j])

    def both_ways(d):
        lists = [chunks_of(sizes[way][d]) for way in (0, 1)]
        return [
            (i, way) + lists[way][i]
            for i in range(max(len(rows) for rows in lists))
            for way in (0, 1) if i < len(lists[way])
        ]

    def rows_out(way, d, lo, n):
        if d == 0:
            return s_ref.at[way, pl.ds(lo, n)]
        return held.at[way, pl.ds(offs[way][d] + lo, n)]

    def ring_copy(way, d, i, lo, n):
        return pltpu.make_async_remote_copy(
            src_ref=rows_out(way, d, lo, n),
            dst_ref=held.at[way, pl.ds(offs[way][d + 1] + lo, n)],
            send_sem=d_send.at[way, d],
            recv_sem=d_recv.at[way, d, i],
            device_id={"ep": onward[way]},
            device_id_type=MESH,
        )

    def meta_copy(way, d):
        return pltpu.make_async_remote_copy(
            src_ref=meta_ref.at[way] if d == 0 else meta_held.at[way, d - 1],
            dst_ref=meta_held.at[way, d],
            send_sem=m_send.at[way, d],
            recv_sem=m_recv.at[way, d],
            device_id={"ep": onward[way]},
            device_id_type=MESH,
        )

    def inbox(way, d, lo, n):
        if d == 0:
            return final.at[way, pl.ds(lo, n)]
        if d <= shared:
            return held.at[way, pl.ds(offs[way][d] + lo, n)]
        return coming.at[way, pl.ds(offs[way][d] - offs[way][shared + 1] + lo, n)]

    def home_copy(way, d, i, lo, n):
        return pltpu.make_async_remote_copy(
            src_ref=inbox(way, d, lo, n),
            dst_ref=inbox(way, d - 1, lo, n),
            send_sem=r_send.at[way, d - 1],
            recv_sem=r_recv.at[way, d - 1, i],
            device_id={"ep": home[way]},
            device_id_type=MESH,
        )

    for j in range(3):
        for copy in (1, 2):
            far_copy(j, copy).start()
    for j in range(3):
        own_weight(j).start()
        pair_copy(j, 0).start()

    tok = out_ref.shape[0]
    tokens_in.wait()
    step = min(64, tok)

    @pl.loop(0, tok // step)
    def _(i):
        at = pl.ds(pl.multiple_of(i * step, step), step)
        values = x_ref[at, :].astype(jnp.float32)
        scale = lax.rsqrt(jnp.mean(values * values, axis=-1, keepdims=True) + 1e-06)
        contrib[0, at, :] = (values * scale * gain_ref[...]).astype(jnp.bfloat16)

    down_at = lax.broadcasted_iota(jnp.int32, (tok, tok), 0)
    across_at = lax.broadcasted_iota(jnp.int32, (tok, tok), 1)
    before_it = down_at < across_at

    def column(row):
        return jnp.sum(jnp.where(down_at == across_at, row, 0.0), axis=1, keepdims=True)

    def count_down(test):
        return jnp.sum(jnp.where(test, 1.0, 0.0), axis=0, keepdims=True)

    ids = [ids_ref[k:k + 1, :].astype(jnp.float32) for k in (0, 1)]
    routes = [route_ref[k:k + 1, :] for k in (0, 1)]
    id_columns = [column(row) for row in ids]
    hosts, targets = ([], [])
    for k in (0, 1):
        named = (id_columns[0] == ids[k]) | (id_columns[1] == ids[k])
        slot = count_down(named & before_it)
        targets.append(ids[k] * slots + slot)
        off = (ids[k] - z.astype(jnp.float32)) * turn.astype(jnp.float32)
        off = jnp.where(off < 0.0, off + ring, off)
        ahead_half = (off < far) | ((off == far) & (slot < opposite_split(slots)))
        signed = jnp.where(ahead_half, off, off - ring)
        hosts.append(
            jnp.where(
                jnp.abs(signed) <= near, signed,
                jnp.where(signed > 0.0, signed - REACH, signed + REACH),
            )
        )
    own_ref[...] = jnp.zeros_like(own_ref)
    for k in (0, 1):
        own_ref[k:k + 1, :] = jnp.where(hosts[k] == 0.0, targets[k], -1.0)
        own_ref[2 + k:3 + k, :] = routes[k]
    for way in (0, 1):
        dist = [host if way == 0 else -host for host in hosts]
        reach = jnp.maximum(jnp.maximum(dist[0], dist[1]), 0.0)
        reach_column = column(reach)
        place = count_down((reach_column > reach) | ((reach_column == reach) & before_it))
        back = jnp.where(column(place) == across_at.astype(jnp.float32), 1.0, 0.0)
        back_ref[way] = back.astype(jnp.bfloat16)
        table = table_ref
        table[...] = jnp.zeros_like(own_ref)
        for k in (0, 1):
            table[k:k + 1, :] = jnp.where(dist[k] > 0.0, targets[k], -1.0)
            table[2 + k:3 + k, :] = routes[k]
        meta_ref[way] = jnp.dot(
            table[...], back, precision=lax.Precision.HIGHEST, preferred_element_type=jnp.float32
        )
        if way == 0:
            sorted_own_ref[...] = jnp.dot(
                own_ref[...], back, precision=lax.Precision.HIGHEST, preferred_element_type=jnp.float32
            )
        pick = jnp.where(place == down_at.astype(jnp.float32), 1.0, 0.0).astype(jnp.bfloat16)
        s_ref[way] = jnp.dot(
            pick, contrib[0], preferred_element_type=jnp.float32
        ).astype(jnp.bfloat16)
        meta_copy(way, 0).start()
        for i, (lo, n) in enumerate(chunks_of(sizes[way][1])):
            ring_copy(way, 0, i, lo, n).start()

    slot_row = lax.broadcasted_iota(jnp.int32, (block, 1), 0).astype(jnp.float32)
    wanted = tuple(
        jnp.where(slot_row < slots, (expert * slots).astype(jnp.float32) + slot_row, -2.0)
        for expert in (z, far_up, far_down)
    )

    def matches(table, copy):
        a = jnp.where(table[0:1, :] == wanted[copy], 1.0, 0.0)
        b = jnp.where(table[1:2, :] == wanted[copy], 1.0, 0.0)
        return a, b

    def table_of(way, d):
        return sorted_own_ref[...] if d == 0 else meta_held[way, d - 1]

    def select(way, d):
        rows = s_ref.shape[1] if d == 0 else sizes[way][d]
        table = table_of(way, d)
        for copy in (0, 1, 2):
            if (copy, way, d) not in places:
                continue
            at = pl.ds(places[(copy, way, d)] * block, block)
            a, b = matches(table, copy)
            scale = jnp.sum(a * table[2:3, :] + b * table[3:4, :], axis=1, keepdims=True)
            one = (a + b).astype(jnp.bfloat16)[:, :rows]
            source = s_ref[0] if d == 0 else held[way, pl.ds(offs[way][d], rows)]
            got = jnp.dot(one, source, preferred_element_type=jnp.float32)
            x_ref[at, :] = got.astype(jnp.bfloat16)
            wj_ref[at, :] = jnp.broadcast_to(scale, (block, wj_ref.shape[1]))

    def ffn(copy, lo_block, hi_block):
        start = (spans[copy] + lo_block) * block
        rows = (hi_block - lo_block) * block
        here = pl.ds(start, rows)
        half = wg.shape[3]
        tile = min(256, half)
        width = x_ref.shape[1]
        cols = min(512, width)

        def widen(part, lo):
            x = x_ref[here, :]
            a = jnp.dot(x, wg[copy, part, :, lo:lo + tile], preferred_element_type=jnp.float32)
            u = jnp.dot(x, wu[copy, part, :, lo:lo + tile], preferred_element_type=jnp.float32)
            h_ref[part, pl.ds(0, rows), lo:lo + tile] = (
                (a / (1.0 + jnp.exp(-a))) * u
            ).astype(jnp.bfloat16)

        def narrow(lo):
            at = slice(lo, lo + cols)
            o = jnp.dot(h_ref[0, pl.ds(0, rows), :], wd[copy, 0, :, at], preferred_element_type=jnp.float32)
            o = o + jnp.dot(h_ref[1, pl.ds(0, rows), :], wd[copy, 1, :, at], preferred_element_type=jnp.float32)
            x_ref[here, at] = (o * wj_ref[here, 0:1]).astype(jnp.bfloat16)

        return [
            functools.partial(widen, part, lo) for part in (0, 1) for lo in range(0, half, tile)
        ] + [functools.partial(narrow, lo) for lo in range(0, width, cols)]

    work = []

    def run(count):
        for piece in work[:count]:
            piece()
        del work[:count]

    def upto(copy, d):
        return len([1 for key in order[copy] if key[1] <= d])

    def spread_weights():
        for j in range(3):
            for copy in (1, 2):
                far_copy(j, copy).wait_recv()

                @pl.loop(1, groups)
                def _(step):
                    side_copy(j, copy, step, g).start()

    def pair_weights():
        for j in range(3):
            for copy in (1, 2):

                @pl.loop(1, groups)
                def _(step):
                    side_copy(j, copy, step, lax.rem(g + groups - step, groups)).wait_recv()

                pair_copy(j, copy).start()

    def finish_weights():
        for j in range(3):
            for copy in (1, 2):
                pair_copy(j, copy).wait()
                far_copy(j, copy).wait_send()

                @pl.loop(1, groups)
                def _(step):
                    side_copy(j, copy, step, g).wait_send()

    select(0, 0)
    cuts = pass_ends(last, near)
    spread_weights()
    for d in range(1, last + 1):
        if d >= 3:
            for way in (0, 1):
                ring_copy(way, d - 3, 0, 0, sizes[way][d - 2]).wait_send()
                meta_copy(way, d - 3).wait_send()
        for way in (0, 1):
            meta_copy(way, d - 1).wait_recv()
            if d < last:
                meta_copy(way, d).start()
        onwards = [dict(chunks_of(sizes[way][d + 1])) for way in (0, 1)]
        for i, way, lo, n in both_ways(d):
            ring_copy(way, d - 1, i, lo, n).wait_recv()
            if lo in onwards[way]:
                ring_copy(way, d, i, lo, onwards[way][lo]).start()
            if way == 1:
                run(3 if d > cuts[1] else 2)
        for way in (0, 1):
            select(way, d)
        if d == near:
            for j in range(3):
                own_weight(j).wait()
                pair_copy(j, 0).wait()
            work.extend(ffn(0, 0, upto(0, near)))
        if d == near + 1:
            pair_weights()
        if d in cuts:
            if d == cuts[0]:
                finish_weights()
            before = max([-1] + [cut for cut in cuts if cut < d])
            for copy in (1, 2):
                work.extend(ffn(copy, upto(copy, before), upto(copy, d)))
    run(len(work))
    for d in (last - 2, last - 1):
        for way in (0, 1):
            ring_copy(way, d, 0, 0, sizes[way][d + 1]).wait_send()
            meta_copy(way, d).wait_send()

    def gathered(table, rows, way, d, at):
        got = None
        for copy in (0, 1, 2):
            if (copy, way, d) not in places:
                continue
            a, b = matches(table, copy)
            one = (a + b).astype(jnp.bfloat16)[:, :rows]
            part = lax.dot_general(
                one, x_ref[pl.ds(places[(copy, way, d)] * block, block), at],
                (((0,), (0,)), ((), ())), preferred_element_type=jnp.float32,
            )
            got = part if got is None else got + part
        return got

    for d in range(last, 0, -1):
        for way in (0, 1):
            got = gathered(meta_held[way, d - 1], sizes[way][d], way, d, slice(None))
            contrib[way, pl.ds(0, sizes[way][d])] = got.astype(jnp.bfloat16)
        arriving = [dict(chunks_of(sizes[way][d + 1])) for way in (0, 1)]
        for i, way, lo, n in both_ways(d):
            m = arriving[way].get(lo, 0)
            if m:
                home_copy(way, d + 1, i, lo, m).wait_recv()
                was = inbox(way, d, lo, m)
                was[...] = (
                    was[...].astype(jnp.float32) + contrib[way, pl.ds(lo, m)].astype(jnp.float32)
                ).astype(jnp.bfloat16)
            if m < n:
                inbox(way, d, lo + m, n - m)[...] = contrib[way, pl.ds(lo + m, n - m)]
            home_copy(way, d, i, lo, n).start()
    for i, way, lo, n in both_ways(1):
        home_copy(way, 1, i, lo, n).wait_recv()

    tok, width = out_ref.shape
    cols = min(512, width)

    @pl.loop(0, width // cols)
    def _(c):
        at = pl.ds(pl.multiple_of(c * cols, cols), cols)
        got = jnp.dot(back_ref[0], final[0, :, at], preferred_element_type=jnp.float32)
        got = got + jnp.dot(back_ref[1], final[1, :, at], preferred_element_type=jnp.float32)
        got = got + gathered(own_ref[...], tok, 0, 0, at)
        out_ref[:, at] = got.astype(out_ref.dtype)

    for d in range(last, 0, -1):
        for way in (0, 1):
            home_copy(way, d, 0, 0, sizes[way][d]).wait_send()


def per_device(tokens, norm_gain, expert_ids, route_weights, w_gate, w_up, w_down):
    tok, width = tokens.shape
    top = expert_ids.shape[1]
    ring = lax.axis_size("ep")
    groups = lax.axis_size("grp")
    experts = w_gate.shape[0] * ring
    slots = 3 * tok * top // (2 * experts)
    far = ring // 2
    last = far - REACH
    near = REACH // 2
    sizes = [prefix_sizes(tok, slots, far, REACH, way) for way in (0, 1)]
    offs = [[0] * (last + 2), [0] * (last + 2)]
    for way in (0, 1):
        for d in range(1, last + 1):
            offs[way][d + 1] = offs[way][d] + -(-sizes[way][d] // 16) * 16
    total = max(offs[0][last + 1], offs[1][last + 1])
    late = max(offs[way][last + 1] - offs[way][last - 3] for way in (0, 1))
    shared = last - 4
    half = w_gate.shape[2]
    block = -(-slots // 16) * 16
    order, places, spans, blocks = block_plan(far, REACH)
    marks = [-1] + list(pass_ends(last, near))
    widest = max(
        len([1 for key in order[copy] if lo < key[1] <= hi])
        for copy in (0, 1, 2) for lo, hi in zip(marks, marks[1:])
    )

    vm = pl.BlockSpec(memory_space=pltpu.VMEM)
    hbm = pl.BlockSpec(memory_space=pl.ANY)
    most = len(chunks_of(tok))
    bf16, f32 = jnp.bfloat16, jnp.float32
    call = pl.pallas_call(
        functools.partial(moe_kernel, ring, groups, slots, sizes, offs, shared),
        out_shape=jax.ShapeDtypeStruct((tok, width), bf16),
        in_specs=[hbm, vm, vm, vm, hbm, hbm, hbm],
        out_specs=vm,
        scratch_shapes=[
            pltpu.VMEM((2, tok, width), bf16),
            pltpu.VMEM((2, 8, tok), f32),
            pltpu.VMEM((8, tok), f32),
            pltpu.VMEM((8, tok), f32),
            pltpu.VMEM((8, tok), f32),
            pltpu.VMEM((2, tok, tok), bf16),
            pltpu.VMEM((2, total, width), bf16),
            pltpu.VMEM((2, last, 8, tok), f32),
            pltpu.VMEM((2, late, width), bf16),
            pltpu.VMEM((2, tok, width), bf16),
            pltpu.VMEM((2, tok, width), bf16),
            pltpu.VMEM((blocks * block, width), bf16),
            pltpu.VMEM((2, widest * block, half), bf16),
            pltpu.VMEM((blocks * block, 128), f32),
            pltpu.VMEM((3, 2, width, half), bf16),
            pltpu.VMEM((3, 2, width, half), bf16),
            pltpu.VMEM((3, 2, half, width), bf16),
            pltpu.SemaphoreType.DMA((2, last)),
            pltpu.SemaphoreType.DMA((2, last, most)),
            pltpu.SemaphoreType.DMA((2, last)),
            pltpu.SemaphoreType.DMA((2, last)),
            pltpu.SemaphoreType.DMA((2, last)),
            pltpu.SemaphoreType.DMA((2, last, most)),
            pltpu.SemaphoreType.DMA,
            pltpu.SemaphoreType.DMA((3,)),
            pltpu.SemaphoreType.DMA((3, 3)),
            pltpu.SemaphoreType.DMA((3, 3)),
            pltpu.SemaphoreType.DMA((2, 3)),
            pltpu.SemaphoreType.DMA((2, 3)),
            pltpu.SemaphoreType.DMA((2, 3, groups)),
            pltpu.SemaphoreType.DMA((2, 3, groups)),
        ],
        compiler_params=pltpu.CompilerParams(
            collective_id=0, has_side_effects=True, vmem_limit_bytes=67043328
        ),
        cost_estimate=pl.CostEstimate(
            flops=12 * tok * top * width * half, bytes_accessed=24 * width * half, transcendentals=0
        ),
    )
    return call(
        tokens, norm_gain.reshape(1, width), expert_ids.T, route_weights.T,
        w_gate, w_up, w_down,
    )


def solution(mesh):
    in_specs = (
        P(("grp", "ep", "tp"), None),
        P(),
        P(("grp", "ep", "tp"), None),
        P(("grp", "ep", "tp"), None),
        P("ep", None, "tp"),
        P("ep", None, "tp"),
        P("ep", "tp", None),
    )
    out_specs = P(("grp", "ep", "tp"), None)
    return jax.shard_map(
        per_device, mesh=mesh, in_specs=in_specs, out_specs=out_specs, check_vma=False
    )
```

```python
import functools

import jax
import jax.numpy as jnp
from jax import lax
from jax.experimental import pallas as pl
from jax.experimental.pallas import tpu as pltpu
from jax.sharding import PartitionSpec as P

MESH = pl.DeviceIdType.MESH
STEPS = (0, 16, 32, 64, 128, 192)
LATE = STEPS[-1]
REACH = 5


def opposite_split(slots):
    return -(-slots // 16) * 8


def prefix_sizes(tok, slots, far, reach, way):
    first = opposite_split(slots)
    at_far = first if way == 0 else slots - first
    last = far - reach
    near = reach // 2
    sizes = [0] * (last + 2)
    for d in range(1, last + 1):
        rows = slots * (last - d) + at_far + 2 * slots * max(0, near - d + 1)
        sizes[d] = -(-min(tok, rows) // 8) * 8
    return sizes


def chunks_of(rows):
    starts = [lo for lo in STEPS if lo < rows]
    return list(zip(starts, [hi - lo for lo, hi in zip(starts, starts[1:] + [rows])]))


def block_plan(far, reach):
    near = reach // 2
    order = {0: [], 1: [], 2: []}
    for d in range(0, far - reach + 1):
        ways = (0,) if d == 0 else (0, 1)
        for way in ways:
            for copy in (0, 1, 2):
                main = d == 0 or copy == 1 + way
                if main or d <= near:
                    order[copy].append((way, d))
    places, at = ({}, 0)
    spans = {}
    for copy in (0, 1, 2):
        spans[copy] = at
        for key in order[copy]:
            places[(copy,) + key] = at
            at += 1
    return order, places, spans, at


def late_reach(sizes):
    return max(d for rows in sizes for d in range(1, len(rows)) if rows[d] > LATE)


def pass_ends(last, late):
    return (late + 3, last - 3, last)


def moe_kernel(
    ring, groups, slots, sizes, offs, shared,
    tok_hbm, gain_ref, ids_ref, route_ref, wg_hbm, wu_hbm, wd_hbm,
    out_ref,
    s_ref, meta_ref, sorted_own_ref, own_ref, table_ref, back_ref, held, meta_held, coming, final, contrib, x_ref, h_ref, wj_ref,
    wg, wu, wd,
    d_send, d_recv, m_send, m_recv, r_send, r_recv,
    tok_local, own_local, pair_send, pair_recv, far_send, far_recv, side_send, side_recv,
):
    g = lax.axis_index("grp")
    z = lax.axis_index("ep")
    core = lax.axis_index("tp")
    far = ring // 2
    last = far - REACH
    near = REACH // 2
    turn = 1 - 2 * core
    up = lax.rem(z + ring + turn, ring)
    down = lax.rem(z + ring - turn, ring)
    far_up = lax.rem(z + ring + turn * REACH, ring)
    far_down = lax.rem(z + ring - turn * REACH, ring)
    onward = (up, down)
    home = (down, up)
    block = -(-slots // 16) * 16
    order, places, spans, _ = block_plan(far, REACH)

    tokens_in = pltpu.make_async_copy(tok_hbm, x_ref.at[pl.ds(0, out_ref.shape[0])], tok_local)
    tokens_in.start()
    barrier = pltpu.get_barrier_semaphore()
    for there in (up, down, far_up, far_down):
        pl.semaphore_signal(barrier, inc=1, device_id={"ep": there}, device_id_type=MESH)
    pl.semaphore_signal(barrier, inc=1, device_id={"tp": 1 - core}, device_id_type=MESH)

    @pl.loop(1, groups)
    def _(j):
        pl.semaphore_signal(
            barrier, inc=1, device_id={"grp": lax.rem(g + j, groups)}, device_id_type=MESH
        )

    pl.semaphore_wait(barrier, 4 + groups)

    weights = ((wg_hbm, wg), (wu_hbm, wu), (wd_hbm, wd))

    def shard(j, which):
        rows = weights[j][0].shape[1] // groups
        return pl.ds(pl.multiple_of(which * rows, rows), rows)

    def far_copy(j, copy):
        src, dst = weights[j]
        return pltpu.make_async_remote_copy(
            src_ref=src.at[0, shard(j, g)],
            dst_ref=dst.at[copy, 0, shard(j, g)],
            send_sem=far_send.at[copy - 1, j],
            recv_sem=far_recv.at[copy - 1, j],
            device_id={"ep": far_down if copy == 1 else far_up},
            device_id_type=MESH,
        )

    def side_copy(j, copy, step, whose):
        ref = weights[j][1].at[copy, 0, shard(j, whose)]
        return pltpu.make_async_remote_copy(
            src_ref=ref, dst_ref=ref,
            send_sem=side_send.at[copy - 1, j, step],
            recv_sem=side_recv.at[copy - 1, j, step],
            device_id={"grp": lax.rem(g + step, groups)},
            device_id_type=MESH,
        )

    def pair_copy(j, copy):
        src, dst = weights[j]
        there = (0, 2, 1)[copy]
        return pltpu.make_async_remote_copy(
            src_ref=src.at[0] if copy == 0 else dst.at[copy, 0],
            dst_ref=dst.at[there, 1],
            send_sem=pair_send.at[copy, j],
            recv_sem=pair_recv.at[there, j],
            device_id={"tp": 1 - core},
            device_id_type=MESH,
        )

    def own_weight(j):
        src, dst = weights[j]
        return pltpu.make_async_copy(src.at[0], dst.at[0, 0], own_local.at[j])

    def both_ways(d):
        lists = [chunks_of(sizes[way][d]) for way in (0, 1)]
        return [
            (i, way) + lists[way][i]
            for i in range(max(len(rows) for rows in lists))
            for way in (0, 1) if i < len(lists[way])
        ]

    def rows_out(way, d, lo, n):
        if d == 0:
            return s_ref.at[way, pl.ds(lo, n)]
        return held.at[way, pl.ds(offs[way][d] + lo, n)]

    def ring_copy(way, d, i, lo, n):
        return pltpu.make_async_remote_copy(
            src_ref=rows_out(way, d, lo, n),
            dst_ref=held.at[way, pl.ds(offs[way][d + 1] + lo, n)],
            send_sem=d_send.at[way, d],
            recv_sem=d_recv.at[way, d, i],
            device_id={"ep": onward[way]},
            device_id_type=MESH,
        )

    def meta_copy(way, d):
        return pltpu.make_async_remote_copy(
            src_ref=meta_ref.at[way] if d == 0 else meta_held.at[way, d - 1],
            dst_ref=meta_held.at[way, d],
            send_sem=m_send.at[way, d],
            recv_sem=m_recv.at[way, d],
            device_id={"ep": onward[way]},
            device_id_type=MESH,
        )

    def inbox(way, d, lo, n):
        if d == 0:
            return final.at[way, pl.ds(lo, n)]
        if d <= shared:
            return held.at[way, pl.ds(offs[way][d] + lo, n)]
        return coming.at[way, pl.ds(offs[way][d] - offs[way][shared + 1] + lo, n)]

    def home_copy(way, d, i, lo, n):
        return pltpu.make_async_remote_copy(
            src_ref=inbox(way, d, lo, n),
            dst_ref=inbox(way, d - 1, lo, n),
            send_sem=r_send.at[way, d - 1],
            recv_sem=r_recv.at[way, d - 1, i],
            device_id={"ep": home[way]},
            device_id_type=MESH,
        )

    for j in range(3):
        for copy in (1, 2):
            far_copy(j, copy).start()
    for j in range(3):
        own_weight(j).start()
        pair_copy(j, 0).start()

    tok = out_ref.shape[0]
    tokens_in.wait()
    step = min(64, tok)

    @pl.loop(0, tok // step)
    def _(i):
        at = pl.ds(pl.multiple_of(i * step, step), step)
        values = x_ref[at, :].astype(jnp.float32)
        scale = lax.rsqrt(jnp.mean(values * values, axis=-1, keepdims=True) + 1e-06)
        contrib[0, at, :] = (values * scale * gain_ref[...]).astype(jnp.bfloat16)

    down_at = lax.broadcasted_iota(jnp.int32, (tok, tok), 0)
    across_at = lax.broadcasted_iota(jnp.int32, (tok, tok), 1)
    before_it = down_at < across_at

    def column(row):
        return jnp.sum(jnp.where(down_at == across_at, row, 0.0), axis=1, keepdims=True)

    def count_down(test):
        return jnp.sum(jnp.where(test, 1.0, 0.0), axis=0, keepdims=True)

    ids = [ids_ref[k:k + 1, :].astype(jnp.float32) for k in (0, 1)]
    routes = [route_ref[k:k + 1, :] for k in (0, 1)]
    id_columns = [column(row) for row in ids]
    hosts, targets = ([], [])
    for k in (0, 1):
        named = (id_columns[0] == ids[k]) | (id_columns[1] == ids[k])
        slot = count_down(named & before_it)
        targets.append(ids[k] * slots + slot)
        off = (ids[k] - z.astype(jnp.float32)) * turn.astype(jnp.float32)
        off = jnp.where(off < 0.0, off + ring, off)
        ahead_half = (off < far) | ((off == far) & (slot < opposite_split(slots)))
        signed = jnp.where(ahead_half, off, off - ring)
        hosts.append(
            jnp.where(
                jnp.abs(signed) <= near, signed,
                jnp.where(signed > 0.0, signed - REACH, signed + REACH),
            )
        )
    own_ref[...] = jnp.zeros_like(own_ref)
    for k in (0, 1):
        own_ref[k:k + 1, :] = jnp.where(hosts[k] == 0.0, targets[k], -1.0)
        own_ref[2 + k:3 + k, :] = routes[k]
    for way in (0, 1):
        dist = [host if way == 0 else -host for host in hosts]
        reach = jnp.maximum(jnp.maximum(dist[0], dist[1]), 0.0)
        reach_column = column(reach)
        place = count_down((reach_column > reach) | ((reach_column == reach) & before_it))
        back = jnp.where(column(place) == across_at.astype(jnp.float32), 1.0, 0.0)
        back_ref[way] = back.astype(jnp.bfloat16)
        table = table_ref
        table[...] = jnp.zeros_like(own_ref)
        for k in (0, 1):
            table[k:k + 1, :] = jnp.where(dist[k] > 0.0, targets[k], -1.0)
            table[2 + k:3 + k, :] = routes[k]
        meta_ref[way] = jnp.dot(
            table[...], back, precision=lax.Precision.HIGHEST, preferred_element_type=jnp.float32
        )
        if way == 0:
            sorted_own_ref[...] = jnp.dot(
                own_ref[...], back, precision=lax.Precision.HIGHEST, preferred_element_type=jnp.float32
            )
        pick = jnp.where(place == down_at.astype(jnp.float32), 1.0, 0.0).astype(jnp.bfloat16)
        s_ref[way] = jnp.dot(
            pick, contrib[0], preferred_element_type=jnp.float32
        ).astype(jnp.bfloat16)
        meta_copy(way, 0).start()
        for i, (lo, n) in enumerate(chunks_of(sizes[way][1])):
            if lo < LATE:
                ring_copy(way, 0, i, lo, n).start()

    slot_row = lax.broadcasted_iota(jnp.int32, (block, 1), 0).astype(jnp.float32)
    wanted = tuple(
        jnp.where(slot_row < slots, (expert * slots).astype(jnp.float32) + slot_row, -2.0)
        for expert in (z, far_up, far_down)
    )

    def matches(table, copy):
        a = jnp.where(table[0:1, :] == wanted[copy], 1.0, 0.0)
        b = jnp.where(table[1:2, :] == wanted[copy], 1.0, 0.0)
        return a, b

    def table_of(way, d):
        return sorted_own_ref[...] if d == 0 else meta_held[way, d - 1]

    def select(way, d):
        rows = s_ref.shape[1] if d == 0 else sizes[way][d]
        table = table_of(way, d)
        for copy in (0, 1, 2):
            if (copy, way, d) not in places:
                continue
            at = pl.ds(places[(copy, way, d)] * block, block)
            a, b = matches(table, copy)
            scale = jnp.sum(a * table[2:3, :] + b * table[3:4, :], axis=1, keepdims=True)
            one = (a + b).astype(jnp.bfloat16)[:, :rows]
            source = s_ref[0] if d == 0 else held[way, pl.ds(offs[way][d], rows)]
            got = jnp.dot(one, source, preferred_element_type=jnp.float32)
            x_ref[at, :] = got.astype(jnp.bfloat16)
            wj_ref[at, :] = jnp.broadcast_to(scale, (block, wj_ref.shape[1]))

    def ffn(copy, lo_block, hi_block):
        start = (spans[copy] + lo_block) * block
        rows = (hi_block - lo_block) * block
        here = pl.ds(start, rows)
        half = wg.shape[3]
        tile = min(256, half)
        width = x_ref.shape[1]
        cols = min(512, width)

        def widen(part, lo):
            x = x_ref[here, :]
            a = jnp.dot(x, wg[copy, part, :, lo:lo + tile], preferred_element_type=jnp.float32)
            u = jnp.dot(x, wu[copy, part, :, lo:lo + tile], preferred_element_type=jnp.float32)
            h_ref[part, pl.ds(0, rows), lo:lo + tile] = (
                (a / (1.0 + jnp.exp(-a))) * u
            ).astype(jnp.bfloat16)

        def narrow(lo):
            at = slice(lo, lo + cols)
            o = jnp.dot(h_ref[0, pl.ds(0, rows), :], wd[copy, 0, :, at], preferred_element_type=jnp.float32)
            o = o + jnp.dot(h_ref[1, pl.ds(0, rows), :], wd[copy, 1, :, at], preferred_element_type=jnp.float32)
            x_ref[here, at] = (o * wj_ref[here, 0:1]).astype(jnp.bfloat16)

        return [
            functools.partial(widen, part, lo) for part in (0, 1) for lo in range(0, half, tile)
        ] + [functools.partial(narrow, lo) for lo in range(0, width, cols)]

    work = []

    def run(count):
        for piece in work[:count]:
            piece()
        del work[:count]

    def upto(copy, d):
        return len([1 for key in order[copy] if key[1] <= d])

    def spread_weights():
        for j in range(3):
            for copy in (1, 2):
                far_copy(j, copy).wait_recv()

                @pl.loop(1, groups)
                def _(step):
                    side_copy(j, copy, step, g).start()

    def pair_weights():
        for j in range(3):
            for copy in (1, 2):

                @pl.loop(1, groups)
                def _(step):
                    side_copy(j, copy, step, lax.rem(g + groups - step, groups)).wait_recv()

                pair_copy(j, copy).start()

    def finish_weights():
        for j in range(3):
            for copy in (1, 2):
                pair_copy(j, copy).wait()
                far_copy(j, copy).wait_send()

                @pl.loop(1, groups)
                def _(step):
                    side_copy(j, copy, step, g).wait_send()

    select(0, 0)
    late = late_reach(sizes)
    cuts = pass_ends(last, late)

    def late_rows(way, d):
        return max(0, sizes[way][d] - LATE)

    def late_hop(d):
        for way in (0, 1):
            if d > 0 and late_rows(way, d):
                ring_copy(way, d - 1, STEPS.index(LATE), LATE, late_rows(way, d)).wait_recv()
            if late_rows(way, d + 1):
                ring_copy(way, d, STEPS.index(LATE), LATE, late_rows(way, d + 1)).start()

    spread_weights()
    for d in range(1, last + 1):
        if d >= 3:
            for way in (0, 1):
                ring_copy(way, d - 3, 0, 0, min(LATE, sizes[way][d - 2])).wait_send()
                meta_copy(way, d - 3).wait_send()
        for way in (0, 1):
            meta_copy(way, d - 1).wait_recv()
            if d < last:
                meta_copy(way, d).start()
        onwards = [dict(chunks_of(sizes[way][d + 1])) for way in (0, 1)]
        for i, way, lo, n in both_ways(d):
            if lo >= LATE:
                continue
            ring_copy(way, d - 1, i, lo, n).wait_recv()
            if lo in onwards[way]:
                ring_copy(way, d, i, lo, onwards[way][lo]).start()
            if way == 1:
                run(3 if d > cuts[1] else 2)
        if d > late:
            for way in (0, 1):
                select(way, d)
        if d == near:
            for j in range(3):
                own_weight(j).wait()
                pair_copy(j, 0).wait()
        if d == near + 1:
            pair_weights()
        if d in cuts:
            if d == cuts[0]:
                finish_weights()
            before = max([late] + [cut for cut in cuts if cut < d])
            for copy in (1, 2):
                work.extend(ffn(copy, upto(copy, before), upto(copy, d)))
        if d == last - 1:
            late_hop(0)
    run(len(work) // 2)
    late_hop(1)
    run(len(work))
    for d in (last - 2, last - 1):
        for way in (0, 1):
            ring_copy(way, d, 0, 0, sizes[way][d + 1]).wait_send()
            meta_copy(way, d).wait_send()

    def gathered(table, rows, way, d, at):
        got = None
        for copy in (0, 1, 2):
            if (copy, way, d) not in places:
                continue
            a, b = matches(table, copy)
            one = (a + b).astype(jnp.bfloat16)[:, :rows]
            part = lax.dot_general(
                one, x_ref[pl.ds(places[(copy, way, d)] * block, block), at],
                (((0,), (0,)), ((), ())), preferred_element_type=jnp.float32,
            )
            got = part if got is None else got + part
        return got

    for d in range(last, 0, -1):
        if d == last - 5:
            run(len(work) - rest)
        if d == late:
            run(len(work))
        for way in (0, 1):
            got = gathered(meta_held[way, d - 1], sizes[way][d], way, d, slice(None))
            contrib[way, pl.ds(0, sizes[way][d])] = got.astype(jnp.bfloat16)
        arriving = [dict(chunks_of(sizes[way][d + 1])) for way in (0, 1)]
        for i, way, lo, n in both_ways(d):
            m = arriving[way].get(lo, 0)
            if m:
                home_copy(way, d + 1, i, lo, m).wait_recv()
                was = inbox(way, d, lo, m)
                was[...] = (
                    was[...].astype(jnp.float32) + contrib[way, pl.ds(lo, m)].astype(jnp.float32)
                ).astype(jnp.bfloat16)
            if m < n:
                inbox(way, d, lo + m, n - m)[...] = contrib[way, pl.ds(lo + m, n - m)]
            home_copy(way, d, i, lo, n).start()
            if way == 1:
                run(2)
        if d == last:
            for hop in range(2, late):
                late_hop(hop)
        if d == last - 1:
            late_hop(late)
            for way in (0, 1):
                for hop in range(0, late):
                    if late_rows(way, hop + 1):
                        ring_copy(way, hop, 0, LATE, late_rows(way, hop + 1)).wait_send()
            for hop in range(1, late + 1):
                work.extend(functools.partial(select, way, hop) for way in (0, 1))
            final_passes = ffn(0, 0, upto(0, near))
            for copy in (1, 2):
                final_passes.extend(ffn(copy, 0, upto(copy, late)))
            rest = len(final_passes)
            work.extend(final_passes)
    for i, way, lo, n in both_ways(1):
        home_copy(way, 1, i, lo, n).wait_recv()

    tok, width = out_ref.shape
    cols = min(512, width)

    @pl.loop(0, width // cols)
    def _(c):
        at = pl.ds(pl.multiple_of(c * cols, cols), cols)
        got = jnp.dot(back_ref[0], final[0, :, at], preferred_element_type=jnp.float32)
        got = got + jnp.dot(back_ref[1], final[1, :, at], preferred_element_type=jnp.float32)
        got = got + gathered(own_ref[...], tok, 0, 0, at)
        out_ref[:, at] = got.astype(out_ref.dtype)

    for d in range(last, 0, -1):
        for way in (0, 1):
            home_copy(way, d, 0, 0, sizes[way][d]).wait_send()


def per_device(tokens, norm_gain, expert_ids, route_weights, w_gate, w_up, w_down):
    tok, width = tokens.shape
    top = expert_ids.shape[1]
    ring = lax.axis_size("ep")
    groups = lax.axis_size("grp")
    experts = w_gate.shape[0] * ring
    slots = 3 * tok * top // (2 * experts)
    far = ring // 2
    last = far - REACH
    near = REACH // 2
    sizes = [prefix_sizes(tok, slots, far, REACH, way) for way in (0, 1)]
    offs = [[0] * (last + 2), [0] * (last + 2)]
    for way in (0, 1):
        for d in range(1, last + 1):
            offs[way][d + 1] = offs[way][d] + -(-sizes[way][d] // 16) * 16
    total = max(offs[0][last + 1], offs[1][last + 1])
    beyond = max(offs[way][last + 1] - offs[way][last - 3] for way in (0, 1))
    shared = last - 4
    half = w_gate.shape[2]
    block = -(-slots // 16) * 16
    order, places, spans, blocks = block_plan(far, REACH)
    late = late_reach(sizes)
    marks = [-1, late] + list(pass_ends(last, late))
    widest = max(
        len([1 for key in order[copy] if lo < key[1] <= hi])
        for copy in (0, 1, 2) for lo, hi in zip(marks, marks[1:])
    )

    vm = pl.BlockSpec(memory_space=pltpu.VMEM)
    hbm = pl.BlockSpec(memory_space=pl.ANY)
    most = len(chunks_of(tok))
    bf16, f32 = jnp.bfloat16, jnp.float32
    call = pl.pallas_call(
        functools.partial(moe_kernel, ring, groups, slots, sizes, offs, shared),
        out_shape=jax.ShapeDtypeStruct((tok, width), bf16),
        in_specs=[hbm, vm, vm, vm, hbm, hbm, hbm],
        out_specs=vm,
        scratch_shapes=[
            pltpu.VMEM((2, tok, width), bf16),
            pltpu.VMEM((2, 8, tok), f32),
            pltpu.VMEM((8, tok), f32),
            pltpu.VMEM((8, tok), f32),
            pltpu.VMEM((8, tok), f32),
            pltpu.VMEM((2, tok, tok), bf16),
            pltpu.VMEM((2, total, width), bf16),
            pltpu.VMEM((2, last, 8, tok), f32),
            pltpu.VMEM((2, beyond, width), bf16),
            pltpu.VMEM((2, tok, width), bf16),
            pltpu.VMEM((2, tok, width), bf16),
            pltpu.VMEM((blocks * block, width), bf16),
            pltpu.VMEM((2, widest * block, half), bf16),
            pltpu.VMEM((blocks * block, 128), f32),
            pltpu.VMEM((3, 2, width, half), bf16),
            pltpu.VMEM((3, 2, width, half), bf16),
            pltpu.VMEM((3, 2, half, width), bf16),
            pltpu.SemaphoreType.DMA((2, last)),
            pltpu.SemaphoreType.DMA((2, last, most)),
            pltpu.SemaphoreType.DMA((2, last)),
            pltpu.SemaphoreType.DMA((2, last)),
            pltpu.SemaphoreType.DMA((2, last)),
            pltpu.SemaphoreType.DMA((2, last, most)),
            pltpu.SemaphoreType.DMA,
            pltpu.SemaphoreType.DMA((3,)),
            pltpu.SemaphoreType.DMA((3, 3)),
            pltpu.SemaphoreType.DMA((3, 3)),
            pltpu.SemaphoreType.DMA((2, 3)),
            pltpu.SemaphoreType.DMA((2, 3)),
            pltpu.SemaphoreType.DMA((2, 3, groups)),
            pltpu.SemaphoreType.DMA((2, 3, groups)),
        ],
        compiler_params=pltpu.CompilerParams(
            collective_id=0, has_side_effects=True, vmem_limit_bytes=67043328
        ),
        cost_estimate=pl.CostEstimate(
            flops=12 * tok * top * width * half, bytes_accessed=24 * width * half, transcendentals=0
        ),
    )
    return call(
        tokens, norm_gain.reshape(1, width), expert_ids.T, route_weights.T,
        w_gate, w_up, w_down,
    )


def solution(mesh):
    in_specs = (
        P(("grp", "ep", "tp"), None),
        P(),
        P(("grp", "ep", "tp"), None),
        P(("grp", "ep", "tp"), None),
        P("ep", None, "tp"),
        P("ep", None, "tp"),
        P("ep", "tp", None),
    )
    out_specs = P(("grp", "ep", "tp"), None)
    return jax.shard_map(
        per_device, mesh=mesh, in_specs=in_specs, out_specs=out_specs, check_vma=False
    )
```
